256 devices in a mesh: sp: 32 (over z, x), tp: 8 (over y, core).
Axes of the slice: x: 4, y: 4, z: 8, core: 2. Of those that a mesh axis runs over, the one named last changes fastest.
Arguments:
- token_grid: bfloat16 [32, 2048, 512], P('sp', 'tp'), may hold values from -6 to 6
- norm_gain: bfloat16 [3, 2048], replicated, may hold values from 0.099609375 to 1.8984375
- w_query: bfloat16 [3, 2048, 2048], P(None, None, 'tp'), may hold values from -0.125 to 0.125
- w_key: bfloat16 [3, 2048, 2048], P(None, None, 'tp'), may hold values from -0.125 to 0.125
- w_value: bfloat16 [3, 2048, 2048], P(None, None, 'tp'), may hold values from -0.125 to 0.125
- w_out: bfloat16 [3, 2048, 2048], P(None, 'tp'), may hold values from -0.5 to 0.5
- rel_bias: float32 [3, 32, 8, 16], P(None, 'tp'), may hold values from -3 to 250
Outputs:
- grid_out: bfloat16 [32, 2048, 512], P('sp', 'tp')
The draws below stay inside these ranges and needn't reach their ends.
All inputs are finite; a program needn't handle non-finite values.
Results may differ from the reference program's by a relative error of at most 0.024.
Values may be sent and summed in bfloat16 or wider, within the bound.
A program may use at most 128 MiB of HBM per device.

```python
import jax
import jax.numpy as jnp
from jax import lax

D = 2048
HEADS = 32
HEAD_DIM = 64
WIN_R = 8
WIN_C = 16
LAYERS = 3
COLS = 512
ROWS = 32
N_TP = 8


def draw_rel_bias(key, part):
    dims_all = (LAYERS, HEADS, WIN_R, WIN_C)
    baseline = jnp.clip(jax.random.normal(jax.random.fold_in(key, 11), dims_all, jnp.float32), -3.0, 3.0)
    return baseline


def block_scale(own_key, shape, shards, low, high):
    def one(axis_at, shards_of):
        steps = jax.random.uniform(jax.random.fold_in(jax.random.fold_in(own_key, 6), axis_at), (shards_of,), jnp.float32, low / len(shards), high / len(shards))
        return jnp.repeat(jnp.exp(steps), shape[axis_at] // shards_of).reshape((-1,) + (1,) * (len(shape) - axis_at - 1))

    factor_of = one(*shards[0])
    for cut in shards[1:]:
        factor_of = factor_of * one(*cut)
    return factor_of


def scatter_about(key, dims, deviation, most, pieces=(), kind=jnp.bfloat16):
    drawn = deviation * jax.random.normal(key, dims, jnp.float32)
    if pieces:
        drawn = drawn * block_scale(key, dims, pieces, -0.22, 0.18)
    return jnp.clip(drawn, -most, most).astype(kind)


def setup_inputs(seed: int = 0) -> dict:
    keys = jax.random.split(jax.random.key(seed), 8)
    return {
        "token_grid": scatter_about(keys[0], (ROWS, D, COLS), 1.0, 6.0, ((0, 32), (1, 8))),
        "norm_gain": jnp.clip(1.0 + 0.18 * jax.random.normal(keys[1], (LAYERS, D), jnp.float32), 0.099609375, 1.8984375).astype(jnp.bfloat16),
        "w_query": scatter_about(keys[2], (LAYERS, D, D), D ** -0.5, 0.125, ((2, 8),)),
        "w_key": scatter_about(keys[3], (LAYERS, D, D), D ** -0.5, 0.125, ((2, 8),)),
        "w_value": scatter_about(keys[4], (LAYERS, D, D), D ** -0.5, 0.125, ((2, 8),)),
        "w_out": scatter_about(keys[5], (LAYERS, D, D), (D // 16) ** -0.5, 0.5, ((1, 8),)),
        "rel_bias": draw_rel_bias(jax.random.fold_in(keys[7], 71), 0),
    }


EPS = 1e-06

def rounded(source):
    return lax.optimization_barrier(source.astype(jnp.bfloat16)).astype(jnp.float32)

def one_layer(token_grid, gain_row, w_query, w_key, w_value, w_out, bias_table):
    grid_wide = token_grid.astype(jnp.float32)
    inverse = lax.rsqrt(lax.optimization_barrier(jnp.mean(grid_wide * grid_wide, axis=1)) + EPS)
    scaled = (grid_wide * gain_row.astype(jnp.float32)[None, :, None]).astype(jnp.bfloat16)
    flat_rows = jnp.transpose(scaled, (0, 2, 1)).reshape(ROWS * COLS, D)
    inverse_flat = inverse.reshape(ROWS * COLS, 1)

    def project(weight):
        product = jnp.dot(flat_rows, weight, preferred_element_type=jnp.float32) * inverse_flat
        return rounded(product).reshape(ROWS, COLS, HEADS, HEAD_DIM)
    queries = project(w_query)
    keys_all = project(w_key)
    values_all = project(w_value)
    factor = HEAD_DIM ** (-0.5)
    offsets = jnp.arange(WIN_R * WIN_C, dtype=jnp.int32)

    def scores_at(offset):
        slot_row = offset // WIN_C
        slot_col = offset % WIN_C
        rolled = jnp.roll(keys_all, (WIN_R // 2 - slot_row, WIN_C // 2 - slot_col), axis=(0, 1))
        offset_bias = lax.dynamic_slice(bias_table, (jnp.int32(0), slot_row, slot_col), (HEADS, 1, 1)).reshape(HEADS)
        return lax.optimization_barrier(jnp.sum(queries * rolled, axis=-1)) * factor + offset_bias
    scores = lax.map(scores_at, offsets)
    weights = rounded(jax.nn.softmax(scores, axis=0))

    def accumulate(running, operands):
        weight_now, offset = operands
        slot_row = offset // WIN_C
        slot_col = offset % WIN_C
        rolled = jnp.roll(values_all, (WIN_R // 2 - slot_row, WIN_C // 2 - slot_col), axis=(0, 1))
        return (running + weight_now[..., None] * rolled, None)
    mixed_out, unused = lax.scan(accumulate, jnp.zeros((ROWS, COLS, HEADS, HEAD_DIM), jnp.float32), (weights, offsets))
    mixed_out = mixed_out.astype(jnp.bfloat16).reshape(ROWS * COLS, N_TP, D // N_TP)
    groups = jnp.moveaxis(mixed_out, 1, 0)
    blocks = w_out.reshape(N_TP, D // N_TP, D)

    def add_group(running, operands):
        partial_value = jnp.dot(operands[0], operands[1], preferred_element_type=jnp.float32)
        return (running + rounded(partial_value), None)
    update, unused = lax.scan(add_group, jnp.zeros((ROWS * COLS, D), jnp.float32), (groups, blocks))
    update = jnp.transpose(update.reshape(ROWS, COLS, D), (0, 2, 1))
    return (grid_wide + update).astype(jnp.bfloat16)

def reference(token_grid, norm_gain, w_query, w_key, w_value, w_out, rel_bias):
    current = token_grid
    for layer_idx in range(LAYERS):
        current = one_layer(current, norm_gain[layer_idx], w_query[layer_idx], w_key[layer_idx], w_value[layer_idx], w_out[layer_idx], rel_bias[layer_idx])
    return current
```

```python
import functools

import jax
import jax.numpy as jnp
from jax import lax
from jax.experimental import pallas as pl
from jax.experimental.pallas import tpu as pltpu
from jax.sharding import PartitionSpec as P

D = 2048
HEADS_DEV = 4
HEAD_DIM = 64
CH = 256
N_TP = 8
WIN_R = 8
WIN_C = 16
LAYERS = 3
ROWS = 32
BLOCK_C = 16
STRIP_C = 8
STRIP = ROWS * STRIP_C
HALF = STRIP // 2
TILE_Q = 64
TILES = STRIP // TILE_Q
EPS = 1e-06
NEG = -1e30
MESH = pl.DeviceIdType.MESH
F32 = jnp.float32
BF16 = jnp.bfloat16


def dot(a, b):
    return lax.dot_general(a, b, (((1,), (0,)), ((), ())), preferred_element_type=F32)


def dot_nt(a, b):
    return lax.dot_general(a, b, (((1,), (1,)), ((), ())), preferred_element_type=F32)


def kernel(
    n_sp, x_ref, gain_ref, base_ref, wq_ref, wk_ref, wv_ref, wo_ref, out_ref,
    wqkv, wout, xg, acc, sq, qs_ref, kv, bias, mixed, part, ssum, own, pd2d, rs_y,
    w_sem, ag_s, ag_r, d_s, d_r, y_s, y_r, h_s, h_r,
):
    tp = lax.axis_index("tp")
    sp = lax.axis_index("sp")
    y, core = tp // 2, tp % 2
    right = ((y + 1) % 4) * 2 + core
    left = ((y + 3) % 4) * 2 + core
    opp = ((y + 2) % 4) * 2 + core
    partner = y * 2 + 1 - core
    flip = 1 - 2 * core
    after = (sp + 1) % n_sp
    before = (sp + n_sp - 1) % n_sp

    barrier = pltpu.get_barrier_semaphore()
    for target in ({"tp": right}, {"tp": left}, {"tp": partner}, {"sp": after}, {"sp": before}):
        pl.semaphore_signal(barrier, inc=1, device_id=target, device_id_type=MESH)

    def weight_copies(l):
        copies = []
        for i, ref in enumerate((wq_ref, wk_ref, wv_ref)):
            copies.append(
                pltpu.make_async_copy(ref.at[l], wqkv.at[l, :, :, pl.ds(i * CH, CH)], w_sem.at[l, i])
            )
        for b in range(N_TP):
            copies.append(
                pltpu.make_async_copy(
                    wo_ref.at[l, :, pl.ds(b * CH, CH)], wout.at[l, b], w_sem.at[l, 3 + b]
                )
            )
        return copies

    for l in range(LAYERS):
        for copy in weight_copies(l):
            copy.start()
    for s in range(2):
        xg[s, tp] = x_ref[s]

    def remote(src, dst, s_sem, r_sem, target):
        return pltpu.make_async_remote_copy(
            src_ref=src, dst_ref=dst, send_sem=s_sem, recv_sem=r_sem,
            device_id=target, device_id_type=MESH,
        )

    first, second = pl.ds(0, HALF), pl.ds(HALF, HALF)
    whole = pl.ds(0, STRIP)
    gather = (
        (tp, first, right), (tp, second, right), (left, first, right),
        (tp, second, left), (tp, first, left), (right, second, left),
        (tp, whole, partner), (left, first, partner), (left, second, partner),
        (right, first, partner), (right, second, partner),
        (opp, first, partner), (opp, second, partner),
    )

    def ag(s, k):
        owner, span, target = gather[k]
        ref = xg.at[s, owner, span]
        return remote(ref, ref, ag_s.at[s, k], ag_r.at[s, k], {"tp": target})

    sides = (opp, right, left, tp)

    def die(s, k):
        return remote(part.at[s, k], pd2d.at[s, k], d_s.at[s, k], d_r.at[s, k], {"tp": partner})

    scatter = (
        (0, first, right), (0, second, left), (1, second, right),
        (2, first, left), (1, first, right), (2, second, left),
    )

    def ring(s, k):
        side, span, target = scatter[k]
        return remote(ssum.at[s, side, span], rs_y.at[s, k], y_s.at[s, k], y_r.at[s, k], {"tp": target})

    def halo(s, par):
        return remote(
            kv.at[par, 1 + s], kv.at[par, 3 * (1 - s)], h_s.at[par, s], h_r.at[par, s],
            {"sp": (sp + 2 * s - 1 + n_sp) % n_sp},
        )

    lane_head = lax.broadcasted_iota(jnp.int32, (TILE_Q, CH), 1) // HEAD_DIM
    head_mask = [(lane_head == h).astype(F32).astype(BF16) for h in range(HEADS_DEV)]

    def start_own(s):
        for k in (0, 3, 6, 1, 4):
            ag(s, k).start()

    def arrive(s, k, *onward):
        ag(s, k).wait_recv()
        for j in onward:
            ag(s, j).start()

    def accumulate(s, l, blocks, fresh):
        total = None
        squares = None
        for b in blocks:
            xb = xg[s, b]
            wide = xb.astype(F32)
            sq_b = wide * wide
            sq_b = sq_b[:, :128] + sq_b[:, 128:]
            squares = sq_b if squares is None else squares + sq_b
            scaled = (wide * gain_ref[l, b]).astype(BF16)
            term = dot(scaled, wqkv[l, b])
            total = term if total is None else total + term
        if fresh:
            acc[...] = total
            sq[...] = squares
        else:
            acc[...] += total
            sq[...] += squares

    def project(s, l, par, mid):
        arrive(s, 0, 2, 7)
        arrive(s, 3, 5, 10)
        mid()
        arrive(s, 6)
        accumulate(s, l, (tp, partner), True)
        arrive(s, 1, 8)
        arrive(s, 4, 9)
        accumulate(s, l, (left, right), False)
        for k in (7, 8, 9, 10):
            arrive(s, k)
        accumulate(s, l, (left + flip, right + flip), False)
        arrive(s, 2, 11)
        arrive(s, 5, 12)
        arrive(s, 11)
        arrive(s, 12)
        accumulate(s, l, (opp, opp + flip), False)
        inverse = lax.rsqrt(jnp.sum(sq[...], axis=1, keepdims=True) / D + EPS)
        kv[par, 1 + s] = (acc[:, CH:] * inverse).astype(BF16)
        halo(s, par).start()
        qs_ref[s] = (acc[:, :CH] * (inverse * HEAD_DIM**-0.5)).astype(BF16)
        for k in range(13):
            ag(s, k).wait_send()

    def window(par, slot, t, lo, hi):
        start = t * TILE_Q - 4 * STRIP_C
        stop = start + 16 * STRIP_C
        if start < 0:
            return jnp.concatenate(
                [kv[par, slot, STRIP + start:, lo:hi], kv[par, slot, :stop, lo:hi]], axis=0
            )
        if stop > STRIP:
            return jnp.concatenate(
                [kv[par, slot, start:, lo:hi], kv[par, slot, : stop - STRIP, lo:hi]], axis=0
            )
        return kv[par, slot, start:stop, lo:hi]

    def attend(s, l, par):
        for t in range(TILES):
            q = qs_ref[s, t * TILE_Q : (t + 1) * TILE_Q, :]
            q_all = jnp.concatenate([q * m for m in head_mask], axis=0)
            table = bias[pl.ds(HEADS_DEV * l, HEADS_DEV)].reshape(HEADS_DEV * TILE_Q, 3 * 128)
            scores = jnp.concatenate(
                [dot_nt(q_all, window(par, s + j, t, 0, CH)) for j in range(3)], axis=1
            ) + table
            highest = jnp.max(scores, axis=1, keepdims=True)
            weights = jnp.exp(scores - highest)
            total = jnp.sum(weights, axis=1, keepdims=True)
            weights = weights.astype(BF16)
            values = jnp.concatenate(
                [window(par, s + j, t, CH, 2 * CH) for j in range(3)], axis=0
            )
            o = dot(weights, values) / total
            out = o[:TILE_Q]
            for h in range(1, HEADS_DEV):
                out = jnp.where(lane_head == h, o[h * TILE_Q : (h + 1) * TILE_Q], out)
            mixed[s, t * TILE_Q : (t + 1) * TILE_Q, :] = out.astype(BF16)

    def send_partner(s, l):
        for k in range(4):
            part[s, k] = dot(mixed[s], wout[l, sides[k] + flip]).astype(BF16)
            die(s, k).start()

    def pair(s, l, k):
        mine = dot(mixed[s], wout[l, sides[k]])
        die(s, k).wait_recv()
        return mine + pd2d[s, k].astype(F32)

    def ring_first(s, l):
        ssum[s, 0] = pair(s, l, 0).astype(BF16)
        ring(s, 0).start()
        ring(s, 1).start()
        ssum[s, 1] = pair(s, l, 1).astype(BF16)
        ring(s, 2).start()
        ssum[s, 2] = pair(s, l, 2).astype(BF16)
        ring(s, 3).start()
        own[s] = pair(s, l, 3) + xg[s, tp].astype(F32)

    def ring_relay(s):
        for k, span in ((0, first), (1, second)):
            ring(s, k).wait_recv()
            side = 1 + k
            ssum[s, side, span] = (
                ssum[s, side, span].astype(F32) + rs_y[s, k].astype(F32)
            ).astype(BF16)
            ring(s, 4 + k).start()

    def ring_last(s):
        for k in (2, 3, 4, 5):
            ring(s, k).wait_recv()
        xg[s, tp, first] = (
            own[s, first] + rs_y[s, 4].astype(F32) + rs_y[s, 3].astype(F32)
        ).astype(BF16)
        xg[s, tp, second] = (
            own[s, second] + rs_y[s, 2].astype(F32) + rs_y[s, 5].astype(F32)
        ).astype(BF16)
        for k in range(4):
            die(s, k).wait_send()
        for k in range(6):
            ring(s, k).wait_send()

    pl.semaphore_wait(barrier, 5)
    start_own(0)

    lane_c = lax.broadcasted_iota(jnp.int32, (8, 128), 1) % STRIP_C
    row_c = lax.broadcasted_iota(jnp.int32, (8, 128), 0)
    nothing = jnp.full((8, 128), NEG, F32)

    def build(i, carry):
        lanes = [jnp.broadcast_to(base_ref[i, pl.ds(j, 1)], (8, 128)) for j in range(2)]
        straight = [pltpu.roll(g, 0, 1, stride=1, stride_axis=0) for g in lanes] + [nothing]
        carried = [nothing] + [pltpu.roll(g, 128 - STRIP_C, 1, stride=1, stride_axis=0) for g in lanes]
        for j in range(3):
            t = jnp.where(lane_c >= row_c, straight[j], carried[j])
            for r in range(8):
                bias[i, r * 8 : (r + 1) * 8, j * 128 : (j + 1) * 128] = (
                    t if r == 0 else pltpu.roll(t, r * STRIP_C, 1)
                )
        return carry

    lax.fori_loop(0, LAYERS * HEADS_DEV, build, 0)

    def layer(l, carry):
        par = l % 2
        f, g = par, 1 - par
        for copy in weight_copies(l):
            copy.wait()
        project(f, l, par, lambda: start_own(g))
        project(g, l, par, lambda: None)
        halo(f, par).wait_recv()
        attend(g, l, par)
        send_partner(g, l)
        halo(g, par).wait_recv()
        attend(f, l, par)
        ring_first(g, l)
        send_partner(f, l)
        ring_relay(g)
        ring_first(f, l)
        ring_last(g)

        @pl.when(l < LAYERS - 1)
        def _():
            start_own(g)

        ring_relay(f)
        ring_last(f)
        halo(f, par).wait_send()
        halo(g, par).wait_send()
        return carry

    lax.fori_loop(0, LAYERS, layer, 0)
    for s in range(2):
        out_ref[s] = xg[s, tp]


def run_layers(n_sp, x, gain, base, wq, wk, wv, wo):
    vmem = pl.BlockSpec(memory_space=pltpu.VMEM)
    hbm = pl.BlockSpec(memory_space=pl.ANY)
    dma = pltpu.SemaphoreType.DMA
    return pl.pallas_call(
        functools.partial(kernel, n_sp),
        out_shape=jax.ShapeDtypeStruct((2, STRIP, CH), BF16),
        in_specs=[vmem, vmem, vmem, hbm, hbm, hbm, hbm],
        out_specs=vmem,
        scratch_shapes=[
            pltpu.VMEM((LAYERS, N_TP, CH, 3 * CH), BF16),
            pltpu.VMEM((LAYERS, N_TP, CH, CH), BF16),
            pltpu.VMEM((2, N_TP, STRIP, CH), BF16),
            pltpu.VMEM((STRIP, 3 * CH), F32),
            pltpu.VMEM((STRIP, 128), F32),
            pltpu.VMEM((2, STRIP, CH), BF16),
            pltpu.VMEM((2, 4, STRIP, 2 * CH), BF16),
            pltpu.VMEM((LAYERS * HEADS_DEV, TILE_Q, 3 * 128), F32),
            pltpu.VMEM((2, STRIP, CH), BF16),
            pltpu.VMEM((2, 4, STRIP, CH), BF16),
            pltpu.VMEM((2, 3, STRIP, CH), BF16),
            pltpu.VMEM((2, STRIP, CH), F32),
            pltpu.VMEM((2, 4, STRIP, CH), BF16),
            pltpu.VMEM((2, 6, HALF, CH), BF16),
            dma((LAYERS, 3 + N_TP)), dma((2, 13)), dma((2, 13)), dma((2, 4)), dma((2, 4)),
            dma((2, 6)), dma((2, 6)), dma((2, 2)), dma((2, 2)),
        ],
        compiler_params=pltpu.CompilerParams(
            collective_id=0, has_side_effects=True, vmem_limit_bytes=60 * 1024 * 1024
        ),
    )(x, gain, base, wq, wk, wv, wo)


def body(token_grid, norm_gain, w_query, w_key, w_value, w_out, rel_bias):
    n_sp = lax.axis_size("sp")
    rows = token_grid.shape[0]
    gain = norm_gain.astype(F32).reshape(LAYERS, N_TP, 1, CH)
    base = rel_bias.reshape(LAYERS * HEADS_DEV, WIN_R, 2, STRIP_C).transpose(0, 2, 1, 3)
    base = base.reshape(LAYERS * HEADS_DEV, 2, WIN_R * STRIP_C)
    base = jnp.pad(base, ((0, 0), (0, 0), (0, 64)), constant_values=NEG)
    wq, wk, wv = (w.reshape(LAYERS, N_TP, CH, CH) for w in (w_query, w_key, w_value))

    x = token_grid.reshape(rows, CH, n_sp, BLOCK_C).transpose(2, 0, 3, 1)
    x = lax.all_to_all(x, "sp", 0, 0, tiled=True)
    x = x.reshape(ROWS, 2, STRIP_C, CH).transpose(1, 0, 2, 3).reshape(2, STRIP, CH)
    x = run_layers(n_sp, x, gain, base, wq, wk, wv, w_out)
    x = x.reshape(2, ROWS, STRIP_C, CH).transpose(1, 0, 2, 3)
    x = x.reshape(n_sp, rows, BLOCK_C, CH)
    x = lax.all_to_all(x, "sp", 0, 0, tiled=True)
    return x.transpose(1, 3, 0, 2).reshape(rows, CH, n_sp * BLOCK_C)


def solution(mesh):
    in_specs = (
        P("sp", "tp", None),
        P(),
        P(None, None, "tp"),
        P(None, None, "tp"),
        P(None, None, "tp"),
        P(None, "tp", None),
        P(None, "tp", None, None),
    )
    out_specs = P("sp", "tp", None)
    return jax.shard_map(body, mesh=mesh, in_specs=in_specs, out_specs=out_specs, check_vma=False)
```

```python
import functools

import jax
import jax.numpy as jnp
from jax import lax
from jax.experimental import pallas as pl
from jax.experimental.pallas import tpu as pltpu
from jax.sharding import PartitionSpec as P

D = 2048
HEADS_DEV = 4
HEAD_DIM = 64
CH = 256
N_TP = 8
WIN_R = 8
WIN_C = 16
LAYERS = 3
ROWS = 32
GROUPS = 4
STRIP_C = 8
TILE = 64
TOK = 2 * TILE
EPS = 1e-06
NEG = -1e30
MESH = pl.DeviceIdType.MESH
F32 = jnp.float32
BF16 = jnp.bfloat16


def dot(a, b):
    return lax.dot_general(a, b, (((1,), (0,)), ((), ())), preferred_element_type=F32)


def dot_nt(a, b):
    return lax.dot_general(a, b, (((1,), (1,)), ((), ())), preferred_element_type=F32)


def kernel(
    n_sp, rows, x_ref, gain_ref, bias_ref, wq_ref, wk_ref, wv_ref, wo_ref, out_ref,
    x_src, x_dst, o_src, o_dst,
    wqkv, wout, gains, pad, bias, xg, acc, sq, qs, kv, mixed, part, ssum, own, pd2d, rs_y,
    w_sem, x_s, x_r, o_s, o_r, ag_s, ag_r, d_s, d_r, y_s, y_r, h_s, h_r,
):
    tp = lax.axis_index("tp")
    sp = lax.axis_index("sp")
    y, core = tp // 2, tp % 2
    right = ((y + 1) % 4) * 2 + core
    left = ((y + 3) % 4) * 2 + core
    opp = ((y + 2) % 4) * 2 + core
    partner = y * 2 + 1 - core
    flip = 1 - 2 * core

    barrier = pltpu.get_barrier_semaphore()
    for target in (right, left, partner):
        pl.semaphore_signal(barrier, inc=1, device_id={"tp": target}, device_id_type=MESH)

    def greet(i, carry):
        pl.semaphore_signal(
            barrier, inc=1, device_id={"sp": (sp + i) % n_sp}, device_id_type=MESH
        )
        return carry

    lax.fori_loop(1, n_sp, greet, 0)

    def weight_copies(l):
        copies = []
        for i, ref in enumerate((wq_ref, wk_ref, wv_ref)):
            copies.append(
                pltpu.make_async_copy(ref.at[l], wqkv.at[l, :, :, pl.ds(i * CH, CH)], w_sem.at[l, i])
            )
        for b in range(N_TP):
            copies.append(
                pltpu.make_async_copy(
                    wo_ref.at[l, :, pl.ds(b * CH, CH)], wout.at[l, b], w_sem.at[l, 3 + b]
                )
            )
        return copies

    for l in range(LAYERS):
        for copy in weight_copies(l):
            copy.start()

    def remote(src, dst, s_sem, r_sem, target):
        return pltpu.make_async_remote_copy(
            src_ref=src, dst_ref=dst, send_sem=s_sem, recv_sem=r_sem,
            device_id=target, device_id_type=MESH,
        )

    for r in range(rows):
        turned = x_ref[r].astype(F32).T
        x_src[:, r] = turned.reshape(n_sp, 2, STRIP_C, CH).astype(BF16)

    def scatter_in(i, carry):
        target = (sp + i) % n_sp
        remote(
            x_src.at[target], x_dst.at[pl.ds(sp * rows, rows)], x_s.at[0], x_r.at[0], {"sp": target}
        ).start()
        return carry

    pl.semaphore_wait(barrier, n_sp + 2)
    lax.fori_loop(1, n_sp, scatter_in, 0)
    x_dst[pl.ds(sp * rows, rows)] = x_src[sp]

    for l in range(LAYERS):
        for b in range(N_TP):
            gains[l, b] = gain_ref[l : l + 1, b * CH : (b + 1) * CH].astype(F32)
    pad[...] = jnp.zeros_like(pad)
    for i in range(LAYERS * HEADS_DEV):
        pad[i, :, :WIN_C] = bias_ref[i // HEADS_DEV, i % HEADS_DEV]
    lane = lax.broadcasted_iota(jnp.int32, (8, 128), 1)
    lane_c = lane % STRIP_C
    row_c = lax.broadcasted_iota(jnp.int32, (8, 128), 0)
    nothing = jnp.full((8, 128), NEG, F32)

    def build(i, carry):
        table = pad[i]
        lanes = []
        for j in range(2):
            piece = table if j == 0 else pltpu.roll(table, 128 - STRIP_C, 1)
            piece = jnp.where(lane < STRIP_C, piece, 0.0)
            piece = pltpu.roll(piece, 0, 1, stride=STRIP_C, stride_axis=0)
            piece = jnp.broadcast_to(jnp.sum(piece, axis=0, keepdims=True), (8, 128))
            lanes.append(jnp.where(lane < WIN_R * STRIP_C, piece, NEG))
        straight = [pltpu.roll(g, 0, 1, stride=1, stride_axis=0) for g in lanes] + [nothing]
        carried = [nothing] + [pltpu.roll(g, 128 - STRIP_C, 1, stride=1, stride_axis=0) for g in lanes]
        for j in range(3):
            t = jnp.where(lane_c >= row_c, straight[j], carried[j])
            for r in range(8):
                bias[i, r * 8 : (r + 1) * 8, j * 128 : (j + 1) * 128] = (
                    t if r == 0 else pltpu.roll(t, r * STRIP_C, 1)
                )
        return carry

    lax.fori_loop(0, LAYERS * HEADS_DEV, build, 0)

    others = (n_sp - 1) * rows
    pltpu.make_async_copy(
        x_dst.at[pl.ds(0, others)], x_dst.at[pl.ds(0, others)], x_r.at[0]
    ).wait()
    for g in range(GROUPS):
        for s in range(2):
            xg[g, tp, s * TILE : (s + 1) * TILE] = (
                x_dst[g * 8 : (g + 1) * 8, s].astype(F32).reshape(TILE, CH).astype(BF16)
            )

    first, second, whole = pl.ds(0, TILE), pl.ds(TILE, TILE), pl.ds(0, TOK)
    gather = (
        (tp, first, right), (tp, second, right), (left, first, right),
        (tp, second, left), (tp, first, left), (right, second, left),
        (tp, whole, partner), (left, first, partner), (left, second, partner),
        (right, first, partner), (right, second, partner),
        (opp, first, partner), (opp, second, partner),
    )

    def ag(g, k):
        owner, span, target = gather[k]
        ref = xg.at[g, owner, span]
        return remote(ref, ref, ag_s.at[g, k], ag_r.at[g, k], {"tp": target})

    sides = (opp, right, left, tp)

    def die(g, k):
        return remote(part.at[g, k], pd2d.at[g, k], d_s.at[g, k], d_r.at[g, k], {"tp": partner})

    scatter = (
        (0, first, right), (0, second, left), (1, second, right),
        (2, first, left), (1, first, right), (2, second, left),
    )

    def ring(g, k):
        side, span, target = scatter[k]
        return remote(ssum.at[g, side, span], rs_y.at[g, k], y_s.at[g, k], y_r.at[g, k], {"tp": target})

    def halo(g, par, s):
        return remote(
            kv.at[par, 1 + s, g], kv.at[par, 3 * (1 - s), g], h_s.at[par, g, s], h_r.at[par, g, s],
            {"sp": (sp + 2 * s - 1 + n_sp) % n_sp},
        )

    lane_head = lax.broadcasted_iota(jnp.int32, (TILE, CH), 1) // HEAD_DIM
    head_mask = [(lane_head == h).astype(F32).astype(BF16) for h in range(HEADS_DEV)]

    def start_own(g):
        for k in (0, 3, 6, 1, 4):
            ag(g, k).start()

    def arrive(g, k, *onward):
        ag(g, k).wait_recv()
        for j in onward:
            ag(g, j).start()

    def accumulate(g, l, blocks, fresh):
        total = None
        squares = None
        for b in blocks:
            wide = xg[g, b].astype(F32)
            sq_b = wide * wide
            sq_b = sq_b[:, :128] + sq_b[:, 128:]
            squares = sq_b if squares is None else squares + sq_b
            term = dot((wide * gains[l, b]).astype(BF16), wqkv[l, b])
            total = term if total is None else total + term
        if fresh:
            acc[g] = total
            sq[g] = squares
        else:
            acc[g] += total
            sq[g] += squares

    def q1(g):
        arrive(g, 0, 2, 7)
        arrive(g, 3, 5, 10)

    def q2(g, l):
        arrive(g, 6)
        accumulate(g, l, (tp, partner), True)
        arrive(g, 1, 8)
        arrive(g, 4, 9)
        accumulate(g, l, (left, right), False)

    def q3(g, l):
        arrive(g, 2, 11)
        arrive(g, 5, 12)
        for k in (7, 8, 9, 10):
            arrive(g, k)
        accumulate(g, l, (left + flip, right + flip), False)

    def q4(g, l, par):
        arrive(g, 11)
        arrive(g, 12)
        accumulate(g, l, (opp, opp + flip), False)
        inverse = lax.rsqrt(jnp.sum(sq[g], axis=1, keepdims=True) / D + EPS)
        for s in range(2):
            piece = slice(s * TILE, (s + 1) * TILE)
            kv[par, 1 + s, g] = (acc[g, piece, CH:] * inverse[piece]).astype(BF16)
            halo(g, par, s).start()
        qs[g] = (acc[g, :, :CH] * (inverse * HEAD_DIM**-0.5)).astype(BF16)
        for k in range(13):
            ag(g, k).wait_send()

    def halo_in(g, par):
        for s in range(2):
            halo(g, par, s).wait_recv()

    def window(par, slot, g, lo):
        up, down = (g + 3) % 4, (g + 1) % 4
        return jnp.concatenate(
            [
                kv[par, slot, up, TILE // 2 :, lo : lo + CH],
                kv[par, slot, g, :, lo : lo + CH],
                kv[par, slot, down, : TILE // 2, lo : lo + CH],
            ],
            axis=0,
        )

    def attend(g, l, par):
        for s in range(2):
            q = qs[g, s * TILE : (s + 1) * TILE, :]
            q_all = jnp.concatenate([q * m for m in head_mask], axis=0)
            table = bias[pl.ds(HEADS_DEV * l, HEADS_DEV)].reshape(HEADS_DEV * TILE, 3 * 128)
            scores = jnp.concatenate(
                [dot_nt(q_all, window(par, s + j, g, 0)) for j in range(3)], axis=1
            ) + table
            highest = jnp.max(scores, axis=1, keepdims=True)
            weights = jnp.exp(scores - highest)
            total = jnp.sum(weights, axis=1, keepdims=True)
            weights = weights.astype(BF16)
            values = jnp.concatenate([window(par, s + j, g, CH) for j in range(3)], axis=0)
            o = dot(weights, values) / total
            out = o[:TILE]
            for h in range(1, HEADS_DEV):
                out = jnp.where(lane_head == h, o[h * TILE : (h + 1) * TILE], out)
            mixed[g, s * TILE : (s + 1) * TILE, :] = out.astype(BF16)

    def p1(g, l):
        for k in range(4):
            part[g, k] = dot(mixed[g], wout[l, sides[k] + flip]).astype(BF16)
            die(g, k).start()

    def pair(g, l, k):
        mine = dot(mixed[g], wout[l, sides[k]])
        die(g, k).wait_recv()
        return mine + pd2d[g, k].astype(F32)

    def p2(g, l):
        ssum[g, 0] = pair(g, l, 0).astype(BF16)
        ring(g, 0).start()
        ring(g, 1).start()
        ssum[g, 1] = pair(g, l, 1).astype(BF16)
        ring(g, 2).start()
        ssum[g, 2] = pair(g, l, 2).astype(BF16)
        ring(g, 3).start()
        own[g] = pair(g, l, 3) + xg[g, tp].astype(F32)

    def p3(g):
        for k, span in ((0, first), (1, second)):
            ring(g, k).wait_recv()
            side = 1 + k
            ssum[g, side, span] = (
                ssum[g, side, span].astype(F32) + rs_y[g, k].astype(F32)
            ).astype(BF16)
            ring(g, 4 + k).start()

    def out_copy(g, r):
        row = 8 * g + r
        return remote(
            o_src.at[row], o_dst.at[sp, row % rows], o_s.at[0], o_r.at[0], {"sp": row // rows}
        )

    def p4(g, l):
        for k in (2, 3, 4, 5):
            ring(g, k).wait_recv()
        top = own[g, first] + rs_y[g, 4].astype(F32) + rs_y[g, 3].astype(F32)
        low = own[g, second] + rs_y[g, 2].astype(F32) + rs_y[g, 5].astype(F32)
        for k in range(4):
            die(g, k).wait_send()
        for k in range(6):
            ring(g, k).wait_send()

        @pl.when(l < LAYERS - 1)
        def _():
            xg[g, tp, first] = top.astype(BF16)
            xg[g, tp, second] = low.astype(BF16)
            start_own(g)

        @pl.when(l == LAYERS - 1)
        def _():
            for s, piece in enumerate((top, low)):
                o_src[pl.ds(8 * g, 8), s] = piece.reshape(8, STRIP_C, CH).astype(BF16)

            def send(r, carry):
                row = 8 * g + r

                @pl.when(row // rows != sp)
                def _():
                    out_copy(g, r).start()

                @pl.when(row // rows == sp)
                def _():
                    o_dst[sp, row % rows] = o_src[row]

                return carry

            lax.fori_loop(0, 8, send, 0)

    start_own(0)
    start_own(1)

    def layer(l, carry):
        par = l % 2
        a, b, c, d = (l % 4, (l + 1) % 4, (l + 2) % 4, (l + 3) % 4)
        for copy in weight_copies(l):
            copy.wait()

        def refill(g):
            @pl.when(l == 0)
            def _():
                start_own(g)

            @pl.when(l > 0)
            def _():
                p4(g, l - 1)

        q1(a)

        @pl.when(l > 0)
        def _():
            p3(d)

        refill(c)
        q1(b)
        q2(a, l)
        refill(d)
        q3(a, l)
        q2(b, l)
        q1(c)
        q4(a, l, par)
        q3(b, l)
        q2(c, l)
        q1(d)
        q4(b, l, par)
        q3(c, l)
        q2(d, l)
        q4(c, l, par)
        halo_in(a, par)
        halo_in(b, par)
        q3(d, l)
        halo_in(c, par)
        attend(b, l, par)
        p1(b, l)
        q4(d, l, par)
        p2(b, l)
        halo_in(d, par)
        attend(c, l, par)
        p1(c, l)
        p3(b)
        p2(c, l)
        attend(d, l, par)
        p1(d, l)
        p4(b, l)
        p3(c)
        p2(d, l)
        attend(a, l, par)
        p1(a, l)
        p4(c, l)
        p3(d)
        p2(a, l)
        for g in range(GROUPS):
            for s in range(2):
                halo(g, par, s).wait_send()
        return carry

    lax.fori_loop(0, LAYERS, layer, 0)
    last = LAYERS - 1
    p3(last % 4)
    p4((last + 3) % 4, last)
    p4(last % 4, last)

    pltpu.make_async_copy(
        x_src.at[pl.ds(0, n_sp - 1)], x_src.at[pl.ds(0, n_sp - 1)], x_s.at[0]
    ).wait()
    gone = ROWS - rows
    pltpu.make_async_copy(o_src.at[pl.ds(0, gone)], o_src.at[pl.ds(0, gone)], o_s.at[0]).wait()
    pltpu.make_async_copy(
        o_dst.at[pl.ds(0, n_sp - 1)], o_dst.at[pl.ds(0, n_sp - 1)], o_r.at[0]
    ).wait()
    for r in range(rows):
        out_ref[r] = o_dst[:, r].astype(F32).reshape(n_sp * WIN_C, CH).T.astype(BF16)


def body(token_grid, norm_gain, w_query, w_key, w_value, w_out, rel_bias):
    n_sp = lax.axis_size("sp")
    rows = token_grid.shape[0]
    wq, wk, wv = (w.reshape(LAYERS, N_TP, CH, CH) for w in (w_query, w_key, w_value))
    vmem = pl.BlockSpec(memory_space=pltpu.VMEM)
    hbm = pl.BlockSpec(memory_space=pl.ANY)
    dma = pltpu.SemaphoreType.DMA
    return pl.pallas_call(
        functools.partial(kernel, n_sp, rows),
        out_shape=jax.ShapeDtypeStruct(token_grid.shape, BF16),
        in_specs=[vmem, vmem, vmem, hbm, hbm, hbm, hbm],
        out_specs=vmem,
        scratch_shapes=[
            pltpu.VMEM((n_sp, rows, 2, STRIP_C, CH), BF16),
            pltpu.VMEM((ROWS, 2, STRIP_C, CH), BF16),
            pltpu.VMEM((ROWS, 2, STRIP_C, CH), BF16),
            pltpu.VMEM((n_sp, rows, 2, STRIP_C, CH), BF16),
            pltpu.VMEM((LAYERS, N_TP, CH, 3 * CH), BF16),
            pltpu.VMEM((LAYERS, N_TP, CH, CH), BF16),
            pltpu.VMEM((LAYERS, N_TP, 1, CH), F32),
            pltpu.VMEM((LAYERS * HEADS_DEV, WIN_R, 128), F32),
            pltpu.VMEM((LAYERS * HEADS_DEV, TILE, 3 * 128), F32),
            pltpu.VMEM((GROUPS, N_TP, TOK, CH), BF16),
            pltpu.VMEM((GROUPS, TOK, 3 * CH), F32),
            pltpu.VMEM((GROUPS, TOK, 128), F32),
            pltpu.VMEM((GROUPS, TOK, CH), BF16),
            pltpu.VMEM((2, 4, GROUPS, TILE, 2 * CH), BF16),
            pltpu.VMEM((GROUPS, TOK, CH), BF16),
            pltpu.VMEM((GROUPS, 4, TOK, CH), BF16),
            pltpu.VMEM((GROUPS, 3, TOK, CH), BF16),
            pltpu.VMEM((GROUPS, TOK, CH), F32),
            pltpu.VMEM((GROUPS, 4, TOK, CH), BF16),
            pltpu.VMEM((GROUPS, 6, TILE, CH), BF16),
            dma((LAYERS, 3 + N_TP)), dma((1,)), dma((1,)), dma((1,)), dma((1,)),
            dma((GROUPS, 13)), dma((GROUPS, 13)), dma((GROUPS, 4)), dma((GROUPS, 4)),
            dma((GROUPS, 6)), dma((GROUPS, 6)), dma((2, GROUPS, 2)), dma((2, GROUPS, 2)),
        ],
        compiler_params=pltpu.CompilerParams(
            collective_id=0, has_side_effects=True, vmem_limit_bytes=60 * 1024 * 1024
        ),
    )(token_grid, norm_gain, rel_bias, wq, wk, wv, w_out)


def solution(mesh):
    in_specs = (
        P("sp", "tp", None),
        P(),
        P(None, None, "tp"),
        P(None, None, "tp"),
        P(None, None, "tp"),
        P(None, "tp", None),
        P(None, "tp", None, None),
    )
    out_specs = P("sp", "tp", None)
    return jax.shard_map(body, mesh=mesh, in_specs=in_specs, out_specs=out_specs, check_vma=False)
```

```python
import functools

import jax
import jax.numpy as jnp
from jax import lax
from jax.experimental import pallas as pl
from jax.experimental.pallas import tpu as pltpu
from jax.sharding import PartitionSpec as P

D = 2048
HEAD_DIM = 64
CH = 256
PAIR = 2 * CH
N_TP = 8
CHIPS = 4
WIN_R = 8
WIN_C = 16
LAYERS = 3
HEADS = 8
ROWS = 32
GROUPS = 4
STRIP_C = 8
TILE = 64
EPS = 1e-06
NEG = -1e30
MESH = pl.DeviceIdType.MESH
F32 = jnp.float32
BF16 = jnp.bfloat16

OWN, RELAY, MINE, SIDES, FAR, ATTEND, PROJECT, ADD, FINISH = range(9)
ORDER = (
    (OWN, 0, 1), (OWN, 0, 3), (OWN, 0, 0), (MINE, 0, 1), (MINE, 0, 3),
    (OWN, 0, 2), (MINE, 0, 0), (MINE, 0, 2), (RELAY, 0, 1), (RELAY, 0, 3),
    (SIDES, 0, 1), (SIDES, 0, 3), (RELAY, 0, 0), (SIDES, 0, 0), (RELAY, 0, 2),
    (FAR, 0, 1), (FAR, 0, 3), (FAR, 0, 0), (SIDES, 0, 2), (FAR, 0, 2),
    (ATTEND, 0, 0), (PROJECT, 0, 0), (ATTEND, 0, 1), (PROJECT, 0, 1), (ATTEND, 0, 3),
    (PROJECT, 0, 3), (ADD, 0, 0), (ATTEND, 0, 2), (PROJECT, 0, 2), (ADD, 0, 1),
    (ADD, 0, 3), (FINISH, 0, 0), (MINE, 1, 0), (ADD, 0, 2), (FINISH, 0, 1),
    (FINISH, 0, 3), (RELAY, 1, 0), (MINE, 1, 1), (MINE, 1, 3), (SIDES, 1, 0),
    (RELAY, 1, 1), (FINISH, 0, 2), (MINE, 1, 2), (RELAY, 1, 3), (SIDES, 1, 1),
    (FAR, 1, 0), (FAR, 1, 1), (RELAY, 1, 2), (SIDES, 1, 3), (SIDES, 1, 2),
    (FAR, 1, 3), (FAR, 1, 2), (ATTEND, 1, 0), (PROJECT, 1, 0), (ATTEND, 1, 2),
    (PROJECT, 1, 2), (ATTEND, 1, 1), (PROJECT, 1, 1), (ADD, 1, 0), (ATTEND, 1, 3),
    (PROJECT, 1, 3), (ADD, 1, 2), (ADD, 1, 1), (FINISH, 1, 0), (MINE, 2, 0),
    (ADD, 1, 3), (FINISH, 1, 2), (MINE, 2, 2), (FINISH, 1, 1), (RELAY, 2, 0),
    (MINE, 2, 1), (SIDES, 2, 0), (RELAY, 2, 2), (FINISH, 1, 3), (MINE, 2, 3),
    (SIDES, 2, 2), (RELAY, 2, 1), (FAR, 2, 0), (FAR, 2, 2), (RELAY, 2, 3),
    (SIDES, 2, 3), (SIDES, 2, 1), (FAR, 2, 1), (FAR, 2, 3), (ATTEND, 2, 1),
    (PROJECT, 2, 1), (ATTEND, 2, 3), (PROJECT, 2, 3), (ATTEND, 2, 2), (PROJECT, 2, 2),
    (ATTEND, 2, 0), (PROJECT, 2, 0), (ADD, 2, 3), (ADD, 2, 1), (ADD, 2, 2),
    (ADD, 2, 0), (FINISH, 2, 3), (FINISH, 2, 1), (FINISH, 2, 2), (FINISH, 2, 0),
)


def dot(a, b):
    return lax.dot_general(a, b, (((1,), (0,)), ((), ())), preferred_element_type=F32)


def dot_nt(a, b):
    return lax.dot_general(a, b, (((1,), (1,)), ((), ())), preferred_element_type=F32)


def kernel(
    n_sp, rows, x_ref, gain_ref, bias_ref, wq_ref, wk_ref, wv_ref, wo_ref, out_ref,
    x_src, x_dst, o_src, o_dst, wqkv, wout, gains, heads, pad, bias,
    xg, acc, sq, qs, kv, mixed, ssum, own, rs_y,
    w_sem, wr_s, wr_r, b_s, b_r, x_s, x_r, o_s, o_r, ag_s, ag_r, y_s, y_r, h_s, h_r,
):
    tp = lax.axis_index("tp")
    sp = lax.axis_index("sp")
    y, core = tp // 2, tp % 2
    right, left, opp = (y + 1) % 4, (y + 3) % 4, (y + 2) % 4
    partner = y * 2 + 1 - core

    barrier = pltpu.get_barrier_semaphore()
    for target in (right * 2 + core, left * 2 + core, partner):
        pl.semaphore_signal(barrier, inc=1, device_id={"tp": target}, device_id_type=MESH)

    def greet(i, carry):
        there = (sp + i) % n_sp
        pl.semaphore_signal(barrier, inc=1, device_id={"sp": there}, device_id_type=MESH)
        pl.semaphore_signal(
            barrier, inc=1, device_id={"sp": there, "tp": partner}, device_id_type=MESH
        )
        return carry

    lax.fori_loop(1, n_sp, greet, 0)

    def remote(src, dst, s_sem, r_sem, target):
        return pltpu.make_async_remote_copy(
            src_ref=src, dst_ref=dst, send_sem=s_sem, recv_sem=r_sem,
            device_id=target, device_id_type=MESH,
        )

    def weight_pairs(l):
        pairs = []
        for i, ref in enumerate((wq_ref, wk_ref, wv_ref)):
            lanes = pl.ds(pl.multiple_of(i * PAIR + core * CH, CH), CH)
            pairs.append((ref.at[l], wqkv.at[l, :, :, lanes]))
        for b in range(CHIPS):
            pairs.append(
                (wo_ref.at[l, :, pl.ds(b * PAIR, PAIR)], wout.at[l, b, pl.ds(core * CH, CH)])
            )
        return pairs

    def weights_here(l, i):
        src, dst = weight_pairs(l)[i]
        return pltpu.make_async_copy(src, dst, w_sem.at[l, i])

    def weights_across(l, i):
        src, dst = weight_pairs(l)[i]
        return remote(src, dst, wr_s.at[l, i], wr_r.at[l, i], {"tp": partner})

    parts = 3 + CHIPS
    for l in range(LAYERS):
        for i in range(parts):
            weights_here(l, i).start()

    for r in range(rows):
        turned = x_ref[r].astype(F32).T.reshape(n_sp, 2, STRIP_C, CH).astype(BF16)
        for c in range(2):
            x_src[:, c, r] = turned[:, c]

    here = pl.ds(sp * rows, rows)

    def scatter_in(i, carry):
        there = (sp + i) % n_sp

        @pl.when(i > 0)
        def _():
            remote(
                x_src.at[there, core], x_dst.at[core, here], x_s.at[0], x_r.at[core], {"sp": there}
            ).start()

        remote(
            x_src.at[there, 1 - core], x_dst.at[core, here], x_s.at[1], x_r.at[core],
            {"sp": there, "tp": partner},
        ).start()
        return carry

    pl.semaphore_wait(barrier, 2 * n_sp + 1)
    lax.fori_loop(0, n_sp, scatter_in, 0)
    bias_copy = remote(bias_ref, heads.at[core], b_s.at[0], b_r.at[0], {"tp": partner})
    bias_copy.start()
    for i in range(parts):
        weights_across(0, i).start()
    x_dst[core, here] = x_src[sp, core]
    heads[core] = bias_ref[...]

    for l in range(LAYERS):
        for b in range(N_TP):
            gains[l, b] = gain_ref[l : l + 1, b * CH : (b + 1) * CH].astype(F32)
    pad[...] = jnp.zeros_like(pad)
    bias_copy.wait()
    for l in range(LAYERS):
        for h in range(HEADS):
            pad[l, h, :, :WIN_C] = heads[h // 4, l, h % 4]
    lane = lax.broadcasted_iota(jnp.int32, (8, 128), 1)
    lane_c = lane % STRIP_C
    row_c = lax.broadcasted_iota(jnp.int32, (8, 128), 0)
    nothing = jnp.full((8, 128), NEG, F32)

    def build(l, carry):
        for h in range(HEADS):
            table = pad[l, h]
            lanes = []
            for j in range(2):
                piece = table if j == 0 else pltpu.roll(table, 128 - STRIP_C, 1)
                piece = jnp.where(lane < STRIP_C, piece, 0.0)
                piece = pltpu.roll(piece, 0, 1, stride=STRIP_C, stride_axis=0)
                piece = jnp.broadcast_to(jnp.sum(piece, axis=0, keepdims=True), (8, 128))
                lanes.append(jnp.where(lane < WIN_R * STRIP_C, piece, NEG))
            straight = [pltpu.roll(g, 0, 1, stride=1, stride_axis=0) for g in lanes] + [nothing]
            carried = [nothing] + [
                pltpu.roll(g, 128 - STRIP_C, 1, stride=1, stride_axis=0) for g in lanes
            ]
            for j in range(3):
                t = jnp.where(lane_c >= row_c, straight[j], carried[j])
                for r in range(8):
                    bias[l, h, r * 8 : (r + 1) * 8, j * 128 : (j + 1) * 128] = (
                        t if r == 0 else pltpu.roll(t, r * STRIP_C, 1)
                    )
        return carry

    lax.fori_loop(0, LAYERS, build, 0)

    most = x_dst.at[core, pl.ds(0, ROWS - rows)]
    pltpu.make_async_copy(most, most, x_r.at[core]).wait()
    rest = x_dst.at[1 - core]
    pltpu.make_async_copy(rest, rest, x_r.at[1 - core]).wait()
    for g in range(GROUPS):
        for h in range(2):
            xg[g, y, h] = (
                x_dst[h, g * 8 : (g + 1) * 8].astype(F32).reshape(TILE, CH).astype(BF16)
            )

    to_right, to_left = right * 2 + core, left * 2 + core
    gather = (
        (y, 0, to_right), (y, 1, to_right), (left, 0, to_right),
        (y, 1, to_left), (y, 0, to_left), (right, 1, to_left),
    )

    def ag(g, k):
        owner, half, target = gather[k]
        ref = xg.at[g, owner, half]
        return remote(ref, ref, ag_s.at[g, k], ag_r.at[g, k], {"tp": target})

    sides = (opp, right, left, y)
    scatter = (
        (0, 0, to_right), (0, 1, to_left), (1, 1, to_right),
        (2, 0, to_left), (1, 0, to_right), (2, 1, to_left),
    )

    def ring(g, k):
        side, half, target = scatter[k]
        return remote(
            ssum.at[g, side, half], rs_y.at[g, k], y_s.at[g, k], y_r.at[g, k], {"tp": target}
        )

    def halo(par, g, k):
        slot = 2 * core if k else 2 * (1 - core)
        target = {"tp": partner}
        if k == 0:
            target["sp"] = (sp + 2 * core - 1 + n_sp) % n_sp
        return remote(kv.at[par, 1, g], kv.at[par, slot, g], h_s.at[par, g, k], h_r.at[par, g, k], target)

    lane_head = lax.broadcasted_iota(jnp.int32, (TILE, CH), 1) // HEAD_DIM
    head_mask = [(lane_head == h).astype(F32).astype(BF16) for h in range(4)]

    def start_own(g):
        for k in (0, 3, 1, 4):
            ag(g, k).start()

    def step_own(l, g):
        start_own(g)

    def step_relay(l, g):
        for k, onward in ((0, 2), (3, 5)):
            ag(g, k).wait_recv()
            ag(g, onward).start()

    def accumulate(l, g, blocks, fresh):
        total = None
        squares = None
        for chip, half in blocks:
            wide = xg[g, chip, half].astype(F32)
            sq_b = wide * wide
            sq_b = sq_b[:, :128] + sq_b[:, 128:]
            squares = sq_b if squares is None else squares + sq_b
            b = chip * 2 + half
            term = dot((wide * gains[l, b]).astype(BF16), wqkv[l, b])
            total = term if total is None else total + term
        if fresh:
            acc[g] = total
            sq[g] = squares
        else:
            acc[g] += total
            sq[g] += squares

    ready = set()

    def weights_in(l, which, parts_of):
        if (l, which) in ready:
            return
        ready.add((l, which))
        for i in parts_of:
            weights_here(l, i).wait()
            weights_across(l, i).wait_recv()

    def step_mine(l, g):
        weights_in(l, 0, range(3))
        accumulate(l, g, ((y, 0), (y, 1)), True)

    def step_sides(l, g):
        ag(g, 1).wait_recv()
        ag(g, 4).wait_recv()
        accumulate(l, g, ((left, 0), (right, 1), (left, 1), (right, 0)), False)

    def step_far(l, g):
        par = l % 2
        ag(g, 2).wait_recv()
        ag(g, 5).wait_recv()
        accumulate(l, g, ((opp, 0), (opp, 1)), False)
        inverse = lax.rsqrt(jnp.sum(sq[g], axis=1, keepdims=True) / D + EPS)
        if l >= 2:
            for k in range(2):
                halo(par, g, k).wait_send()
        kv[par, 1, g] = (acc[g, :, PAIR:] * inverse).astype(BF16)
        for k in range(2):
            halo(par, g, k).start()
        qs[g] = (acc[g, :, :PAIR] * (inverse * HEAD_DIM**-0.5)).astype(BF16)
        for k in range(6):
            ag(g, k).wait_send()

    def window(par, slot, g, lo):
        up, down = (g + 3) % 4, (g + 1) % 4
        return jnp.concatenate(
            [
                kv[par, slot, up, TILE // 2 :, lo : lo + CH],
                kv[par, slot, g, :, lo : lo + CH],
                kv[par, slot, down, : TILE // 2, lo : lo + CH],
            ],
            axis=0,
        )

    def step_attend(l, g):
        par = l % 2
        for near in ((g + 3) % 4, g, (g + 1) % 4):
            if (l, near, "halo") not in ready:
                ready.add((l, near, "halo"))
                for k in range(2):
                    halo(par, near, k).wait_recv()
        for c in range(2):
            lo = c * CH
            q = qs[g, :, lo : lo + CH]
            q_all = jnp.concatenate([q * m for m in head_mask], axis=0)
            table = bias[l, 4 * c : 4 * c + 4].reshape(4 * TILE, 3 * 128)
            scores = jnp.concatenate(
                [dot_nt(q_all, window(par, j, g, lo)) for j in range(3)], axis=1
            ) + table
            highest = jnp.max(scores, axis=1, keepdims=True)
            weights = jnp.exp(scores - highest)
            total = jnp.sum(weights, axis=1, keepdims=True)
            weights = weights.astype(BF16)
            values = jnp.concatenate([window(par, j, g, PAIR + lo) for j in range(3)], axis=0)
            o = dot(weights, values) / total
            out = o[:TILE]
            for h in range(1, 4):
                out = jnp.where(lane_head == h, o[h * TILE : (h + 1) * TILE], out)
            mixed[g, :, lo : lo + CH] = out.astype(BF16)
        if l < LAYERS - 1 and (l, "across") not in ready:
            ready.add((l, "across"))
            for i in range(parts):
                weights_across(l + 1, i).start()

    def step_project(l, g):
        weights_in(l, 1, range(3, parts))
        m = mixed[g]
        for k in range(3):
            piece = dot(m, wout[l, sides[k]]).astype(BF16)
            for half in range(2):
                ssum[g, k, half] = piece[:, half * CH : (half + 1) * CH]
        for k in range(4):
            ring(g, k).start()
        piece = dot(m, wout[l, y])
        for half in range(2):
            own[g, half] = piece[:, half * CH : (half + 1) * CH] + xg[g, y, half].astype(F32)

    def step_add(l, g):
        for k in range(2):
            ring(g, k).wait_recv()
            side = 1 + k
            ssum[g, side, k] = (ssum[g, side, k].astype(F32) + rs_y[g, k].astype(F32)).astype(BF16)
            ring(g, 4 + k).start()

    def step_finish(l, g):
        for k in (2, 3, 4, 5):
            ring(g, k).wait_recv()
        new = (
            own[g, 0] + rs_y[g, 4].astype(F32) + rs_y[g, 3].astype(F32),
            own[g, 1] + rs_y[g, 2].astype(F32) + rs_y[g, 5].astype(F32),
        )
        if l < LAYERS - 1:
            for half in range(2):
                xg[g, y, half] = new[half].astype(BF16)
            start_own(g)
        else:
            for half in range(2):
                o_src[half, 8 * g : 8 * g + 8] = new[half].reshape(8, STRIP_C, CH).astype(BF16)

            def send(r, carry):
                row = 8 * g + r
                there, spot = row // rows, row % rows

                @pl.when(there != sp)
                def _():
                    remote(
                        o_src.at[core, row], o_dst.at[core, sp, spot], o_s.at[0], o_r.at[core],
                        {"sp": there},
                    ).start()

                @pl.when(there == sp)
                def _():
                    o_dst[core, sp, spot] = o_src[core, row]

                remote(
                    o_src.at[1 - core, row], o_dst.at[core, sp, spot], o_s.at[1], o_r.at[core],
                    {"sp": there, "tp": partner},
                ).start()
                return carry

            lax.fori_loop(0, 8, send, 0)
        for k in range(6):
            ring(g, k).wait_send()

    steps = (
        step_own, step_relay, step_mine, step_sides, step_far,
        step_attend, step_project, step_add, step_finish,
    )
    for step, l, g in ORDER:
        steps[step](l, g)

    for l in range(LAYERS):
        for i in range(parts):
            weights_across(l, i).wait_send()
    for l in range(1, LAYERS):
        for g in range(GROUPS):
            for k in range(2):
                halo(l % 2, g, k).wait_send()
    gone = x_src.at[pl.ds(0, n_sp - 1), core]
    pltpu.make_async_copy(gone, gone, x_s.at[0]).wait()
    gone = x_src.at[:, core]
    pltpu.make_async_copy(gone, gone, x_s.at[1]).wait()
    gone = o_src.at[core, pl.ds(0, ROWS - rows)]
    pltpu.make_async_copy(gone, gone, o_s.at[0]).wait()
    gone = o_src.at[1 - core]
    pltpu.make_async_copy(gone, gone, o_s.at[1]).wait()
    most = o_dst.at[core, pl.ds(0, n_sp - 1)]
    pltpu.make_async_copy(most, most, o_r.at[core]).wait()
    rest = o_dst.at[1 - core]
    pltpu.make_async_copy(rest, rest, o_r.at[1 - core]).wait()
    for r in range(rows):
        both = jnp.stack([o_dst[c, :, r].astype(F32) for c in range(2)], axis=1)
        out_ref[r] = both.reshape(n_sp * WIN_C, CH).T.astype(BF16)


def body(token_grid, norm_gain, w_query, w_key, w_value, w_out, rel_bias):
    n_sp = lax.axis_size("sp")
    rows = token_grid.shape[0]
    wq, wk, wv = (w.reshape(LAYERS, N_TP, CH, CH) for w in (w_query, w_key, w_value))
    vmem = pl.BlockSpec(memory_space=pltpu.VMEM)
    hbm = pl.BlockSpec(memory_space=pl.ANY)
    dma = pltpu.SemaphoreType.DMA
    parts = 3 + CHIPS
    return pl.pallas_call(
        functools.partial(kernel, n_sp, rows),
        out_shape=jax.ShapeDtypeStruct(token_grid.shape, BF16),
        in_specs=[vmem, vmem, vmem, hbm, hbm, hbm, hbm],
        out_specs=vmem,
        scratch_shapes=[
            pltpu.VMEM((n_sp, 2, rows, STRIP_C, CH), BF16),
            pltpu.VMEM((2, ROWS, STRIP_C, CH), BF16),
            pltpu.VMEM((2, ROWS, STRIP_C, CH), BF16),
            pltpu.VMEM((2, n_sp, rows, STRIP_C, CH), BF16),
            pltpu.VMEM((LAYERS, N_TP, CH, 3 * PAIR), BF16),
            pltpu.VMEM((LAYERS, CHIPS, PAIR, PAIR), BF16),
            pltpu.VMEM((LAYERS, N_TP, 1, CH), F32),
            pltpu.VMEM((2, LAYERS, 4, WIN_R, WIN_C), F32),
            pltpu.VMEM((LAYERS, HEADS, WIN_R, 128), F32),
            pltpu.VMEM((LAYERS, HEADS, TILE, 3 * 128), F32),
            pltpu.VMEM((GROUPS, CHIPS, 2, TILE, CH), BF16),
            pltpu.VMEM((GROUPS, TILE, 3 * PAIR), F32),
            pltpu.VMEM((GROUPS, TILE, 128), F32),
            pltpu.VMEM((GROUPS, TILE, PAIR), BF16),
            pltpu.VMEM((2, 3, GROUPS, TILE, 2 * PAIR), BF16),
            pltpu.VMEM((GROUPS, TILE, PAIR), BF16),
            pltpu.VMEM((GROUPS, 3, 2, TILE, CH), BF16),
            pltpu.VMEM((GROUPS, 2, TILE, CH), F32),
            pltpu.VMEM((GROUPS, 6, TILE, CH), BF16),
            dma((LAYERS, parts)), dma((LAYERS, parts)), dma((LAYERS, parts)),
            dma((1,)), dma((1,)), dma((2,)), dma((2,)), dma((2,)), dma((2,)),
            dma((GROUPS, 6)), dma((GROUPS, 6)), dma((GROUPS, 6)), dma((GROUPS, 6)),
            dma((2, GROUPS, 2)), dma((2, GROUPS, 2)),
        ],
        compiler_params=pltpu.CompilerParams(
            collective_id=0, has_side_effects=True, vmem_limit_bytes=60 * 1024 * 1024
        ),
    )(token_grid, norm_gain, rel_bias, wq, wk, wv, w_out)


def solution(mesh):
    in_specs = (
        P("sp", "tp", None),
        P(),
        P(None, None, "tp"),
        P(None, None, "tp"),
        P(None, None, "tp"),
        P(None, "tp", None),
        P(None, "tp", None, None),
    )
    out_specs = P("sp", "tp", None)
    return jax.shard_map(body, mesh=mesh, in_specs=in_specs, out_specs=out_specs, check_vma=False)
```

```python
import functools

import jax
import jax.numpy as jnp
from jax import lax
from jax.experimental import pallas as pl
from jax.experimental.pallas import tpu as pltpu
from jax.sharding import PartitionSpec as P

D = 2048
HEAD_DIM = 64
CH = 256
PAIR = 2 * CH
N_TP = 8
CHIPS = 4
WIN_R = 8
WIN_C = 16
LAYERS = 3
HEADS = 8
ROWS = 32
GROUPS = 4
STRIP_C = 8
TILE = 64
EPS = 1e-06
NEG = -1e30
MESH = pl.DeviceIdType.MESH
F32 = jnp.float32
BF16 = jnp.bfloat16

OWN, RELAY, MINE, SIDES, FAR, ATTEND, FIRST, REST, ADD, FINISH = range(10)
ORDER = (
    (OWN, 0, 2), (OWN, 0, 3), (OWN, 0, 0), (OWN, 0, 1), (MINE, 0, 2),
    (MINE, 0, 3), (MINE, 0, 0), (RELAY, 0, 2), (SIDES, 0, 2), (RELAY, 0, 3),
    (SIDES, 0, 3), (RELAY, 0, 0), (SIDES, 0, 0), (RELAY, 0, 1), (MINE, 0, 1),
    (SIDES, 0, 1), (FAR, 0, 2), (FAR, 0, 3), (FAR, 0, 0), (FAR, 0, 1),
    (ATTEND, 0, 2), (FIRST, 0, 2), (REST, 0, 2), (ATTEND, 0, 3), (FIRST, 0, 3),
    (REST, 0, 3), (ATTEND, 0, 0), (FIRST, 0, 0), (ADD, 0, 2), (REST, 0, 0),
    (ATTEND, 0, 1), (FIRST, 0, 1), (ADD, 0, 3), (REST, 0, 1), (ADD, 0, 0),
    (FINISH, 0, 2), (MINE, 1, 2), (ADD, 0, 1), (FINISH, 0, 3), (MINE, 1, 3),
    (RELAY, 1, 2), (FINISH, 0, 0), (MINE, 1, 0), (SIDES, 1, 2), (RELAY, 1, 3),
    (FINISH, 0, 1), (SIDES, 1, 3), (FAR, 1, 2), (RELAY, 1, 0), (SIDES, 1, 0),
    (FAR, 1, 3), (RELAY, 1, 1), (FAR, 1, 0), (MINE, 1, 1), (SIDES, 1, 1),
    (FAR, 1, 1), (ATTEND, 1, 2), (FIRST, 1, 2), (REST, 1, 2), (ATTEND, 1, 3),
    (FIRST, 1, 3), (REST, 1, 3), (ADD, 1, 2), (ATTEND, 1, 0), (FIRST, 1, 0),
    (REST, 1, 0), (ADD, 1, 3), (ATTEND, 1, 1), (FIRST, 1, 1), (FINISH, 1, 2),
    (MINE, 2, 2), (ADD, 1, 0), (REST, 1, 1), (FINISH, 1, 3), (ADD, 1, 1),
    (MINE, 2, 3), (RELAY, 2, 2), (FINISH, 1, 0), (MINE, 2, 0), (SIDES, 2, 2),
    (RELAY, 2, 3), (FINISH, 1, 1), (MINE, 2, 1), (FAR, 2, 2), (RELAY, 2, 0),
    (SIDES, 2, 3), (SIDES, 2, 0), (RELAY, 2, 1), (FAR, 2, 3), (SIDES, 2, 1),
    (FAR, 2, 0), (FAR, 2, 1), (ATTEND, 2, 2), (FIRST, 2, 2), (REST, 2, 2),
    (ATTEND, 2, 3), (FIRST, 2, 3), (REST, 2, 3), (ATTEND, 2, 0), (FIRST, 2, 0),
    (REST, 2, 0), (ATTEND, 2, 1), (FIRST, 2, 1), (REST, 2, 1), (ADD, 2, 2),
    (ADD, 2, 3), (ADD, 2, 0), (ADD, 2, 1), (FINISH, 2, 2), (FINISH, 2, 3),
    (FINISH, 2, 0), (FINISH, 2, 1),
)


def dot(a, b):
    return lax.dot_general(a, b, (((1,), (0,)), ((), ())), preferred_element_type=F32)


def dot_nt(a, b):
    return lax.dot_general(a, b, (((1,), (1,)), ((), ())), preferred_element_type=F32)


def kernel(
    n_sp, rows, x_ref, gain_ref, bias_ref, wq_ref, wk_ref, wv_ref, wo_ref, out_ref,
    x_src, x_dst, o_src, o_dst, wqkv, wout, gains, heads, pad, bias,
    xg, acc, sq, qs, kv, mixed, ssum, own, rs_y,
    w_sem, wr_s, wr_r, b_s, b_r, x_s, x_r, o_s, o_r, ag_s, ag_r, y_s, y_r, h_s, h_r,
):
    tp = lax.axis_index("tp")
    sp = lax.axis_index("sp")
    y, core = tp // 2, tp % 2
    right, left, opp = (y + 1) % 4, (y + 3) % 4, (y + 2) % 4
    partner = y * 2 + 1 - core

    barrier = pltpu.get_barrier_semaphore()
    for target in (right * 2 + core, left * 2 + core, partner):
        pl.semaphore_signal(barrier, inc=1, device_id={"tp": target}, device_id_type=MESH)

    def greet(i, carry):
        there = (sp + i) % n_sp
        pl.semaphore_signal(barrier, inc=1, device_id={"sp": there}, device_id_type=MESH)
        pl.semaphore_signal(
            barrier, inc=1, device_id={"sp": there, "tp": partner}, device_id_type=MESH
        )
        return carry

    lax.fori_loop(1, n_sp, greet, 0)

    def remote(src, dst, s_sem, r_sem, target):
        return pltpu.make_async_remote_copy(
            src_ref=src, dst_ref=dst, send_sem=s_sem, recv_sem=r_sem,
            device_id=target, device_id_type=MESH,
        )

    def weight_pairs(l):
        pairs = []
        for i, ref in enumerate((wq_ref, wk_ref, wv_ref)):
            lanes = pl.ds(pl.multiple_of(i * PAIR + core * CH, CH), CH)
            pairs.append((ref.at[l], wqkv.at[l, :, :, lanes]))
        for b in range(CHIPS):
            pairs.append(
                (wo_ref.at[l, :, pl.ds(b * PAIR, PAIR)], wout.at[l, b, pl.ds(core * CH, CH)])
            )
        return pairs

    def weights_here(l, i):
        src, dst = weight_pairs(l)[i]
        return pltpu.make_async_copy(src, dst, w_sem.at[l, i])

    def weights_across(l, i):
        src, dst = weight_pairs(l)[i]
        return remote(src, dst, wr_s.at[l, i], wr_r.at[l, i], {"tp": partner})

    parts = 3 + CHIPS
    for l in range(LAYERS):
        for i in range(parts):
            weights_here(l, i).start()

    for r in range(rows):
        turned = x_ref[r].astype(F32).T.reshape(n_sp, 2, STRIP_C, CH).astype(BF16)
        for c in range(2):
            x_src[:, c, r] = turned[:, c]

    here = pl.ds(sp * rows, rows)

    def scatter_in(i, carry):
        there = (sp + i) % n_sp

        @pl.when(i > 0)
        def _():
            remote(
                x_src.at[there, core], x_dst.at[core, here], x_s.at[0], x_r.at[core], {"sp": there}
            ).start()

        remote(
            x_src.at[there, 1 - core], x_dst.at[core, here], x_s.at[1], x_r.at[core],
            {"sp": there, "tp": partner},
        ).start()
        return carry

    pl.semaphore_wait(barrier, 2 * n_sp + 1)
    lax.fori_loop(0, n_sp, scatter_in, 0)
    bias_copy = remote(bias_ref, heads.at[core], b_s.at[0], b_r.at[0], {"tp": partner})
    bias_copy.start()
    for i in range(parts):
        weights_across(0, i).start()
    x_dst[core, here] = x_src[sp, core]
    heads[core] = bias_ref[...]

    for l in range(LAYERS):
        for b in range(N_TP):
            gains[l, b] = gain_ref[l : l + 1, b * CH : (b + 1) * CH].astype(F32)
    pad[...] = jnp.zeros_like(pad)
    bias_copy.wait()
    for l in range(LAYERS):
        for h in range(HEADS):
            pad[l, h, :, :WIN_C] = heads[h // 4, l, h % 4]
    lane = lax.broadcasted_iota(jnp.int32, (8, 128), 1)
    lane_c = lane % STRIP_C
    row_c = lax.broadcasted_iota(jnp.int32, (8, 128), 0)
    nothing = jnp.full((8, 128), NEG, F32)

    def build(l, carry):
        for h in range(HEADS):
            table = pad[l, h]
            lanes = []
            for j in range(2):
                piece = table if j == 0 else pltpu.roll(table, 128 - STRIP_C, 1)
                piece = jnp.where(lane < STRIP_C, piece, 0.0)
                piece = pltpu.roll(piece, 0, 1, stride=STRIP_C, stride_axis=0)
                piece = jnp.broadcast_to(jnp.sum(piece, axis=0, keepdims=True), (8, 128))
                lanes.append(jnp.where(lane < WIN_R * STRIP_C, piece, NEG))
            straight = [pltpu.roll(g, 0, 1, stride=1, stride_axis=0) for g in lanes] + [nothing]
            carried = [nothing] + [
                pltpu.roll(g, 128 - STRIP_C, 1, stride=1, stride_axis=0) for g in lanes
            ]
            for j in range(3):
                t = jnp.where(lane_c >= row_c, straight[j], carried[j])
                for r in range(8):
                    bias[l, h, r * 8 : (r + 1) * 8, j * 128 : (j + 1) * 128] = (
                        t if r == 0 else pltpu.roll(t, r * STRIP_C, 1)
                    )
        return carry

    lax.fori_loop(0, LAYERS, build, 0)

    most = x_dst.at[core, pl.ds(0, ROWS - rows)]
    pltpu.make_async_copy(most, most, x_r.at[core]).wait()
    rest = x_dst.at[1 - core]
    pltpu.make_async_copy(rest, rest, x_r.at[1 - core]).wait()
    for g in range(GROUPS):
        for h in range(2):
            xg[0, g, y, h] = (
                x_dst[h, g * 8 : (g + 1) * 8].astype(F32).reshape(TILE, CH).astype(BF16)
            )

    to_right, to_left = right * 2 + core, left * 2 + core
    gather = (
        (y, 0, to_right), (y, 1, to_right), (left, 0, to_right),
        (y, 1, to_left), (y, 0, to_left), (right, 1, to_left),
    )

    def ag(l, g, k):
        owner, half, target = gather[k]
        ref = xg.at[l, g, owner, half]
        return remote(ref, ref, ag_s.at[g, k], ag_r.at[g, k], {"tp": target})

    sides = (opp, right, left, y)
    scatter = (
        (0, 0, to_right), (0, 1, to_left), (1, 1, to_right),
        (2, 0, to_left), (1, 0, to_right), (2, 1, to_left),
    )

    def ring(g, k):
        side, half, target = scatter[k]
        return remote(
            ssum.at[g, side, half], rs_y.at[g, k], y_s.at[g, k], y_r.at[g, k], {"tp": target}
        )

    def halo(l, g, k):
        slot = 2 * core if k else 2 * (1 - core)
        target = {"tp": partner}
        if k == 0:
            target["sp"] = (sp + 2 * core - 1 + n_sp) % n_sp
        return remote(kv.at[l, 1, g], kv.at[l, slot, g], h_s.at[l, g, k], h_r.at[l, g, k], target)

    lane_head = lax.broadcasted_iota(jnp.int32, (TILE, CH), 1) // HEAD_DIM
    head_mask = [(lane_head == h).astype(F32).astype(BF16) for h in range(4)]

    def step_own(l, g):
        for k in (0, 3, 1, 4):
            ag(l, g, k).start()

    def step_relay(l, g):
        for k, onward in ((0, 2), (3, 5)):
            ag(l, g, k).wait_recv()
            ag(l, g, onward).start()

    def accumulate(l, g, blocks, fresh):
        total = None
        squares = None
        for chip, half in blocks:
            wide = xg[l, g, chip, half].astype(F32)
            sq_b = wide * wide
            sq_b = sq_b[:, :128] + sq_b[:, 128:]
            squares = sq_b if squares is None else squares + sq_b
            b = chip * 2 + half
            term = dot((wide * gains[l, b]).astype(BF16), wqkv[l, b])
            total = term if total is None else total + term
        if fresh:
            acc[g] = total
            sq[g] = squares
        else:
            acc[g] += total
            sq[g] += squares

    ready = set()

    def weights_in(l, which, parts_of):
        if (l, which) in ready:
            return
        ready.add((l, which))
        for i in parts_of:
            weights_here(l, i).wait()
            weights_across(l, i).wait_recv()

    def step_mine(l, g):
        weights_in(l, 0, range(3))
        accumulate(l, g, ((y, 0), (y, 1)), True)

    def step_sides(l, g):
        ag(l, g, 1).wait_recv()
        ag(l, g, 4).wait_recv()
        accumulate(l, g, ((left, 0), (right, 1), (left, 1), (right, 0)), False)

    def step_far(l, g):
        ag(l, g, 2).wait_recv()
        ag(l, g, 5).wait_recv()
        squares = sq[g]
        scaled = []
        for half in range(2):
            wide = xg[l, g, opp, half].astype(F32)
            scaled.append((wide * gains[l, opp * 2 + half]).astype(BF16))
            wide = wide * wide
            squares = squares + wide[:, :128] + wide[:, 128:]
        inverse = lax.rsqrt(jnp.sum(squares, axis=1, keepdims=True) / D + EPS)

        def total(lo, hi):
            return acc[g, :, lo:hi] + (
                dot(scaled[0], wqkv[l, opp * 2, :, lo:hi])
                + dot(scaled[1], wqkv[l, opp * 2 + 1, :, lo:hi])
            )

        kv[l, 1, g] = (total(PAIR, 3 * PAIR) * inverse).astype(BF16)
        for k in range(2):
            halo(l, g, k).start()
        qs[g] = (total(0, PAIR) * (inverse * HEAD_DIM**-0.5)).astype(BF16)
        for k in range(6):
            ag(l, g, k).wait_send()

    def window(l, slot, g, lo):
        return jnp.concatenate(
            [kv[l, slot, g, :, lo : lo + CH], kv[l, slot, (g + 1) % 4, :, lo : lo + CH]], axis=0
        )

    def step_attend(l, g):
        after = (g + 1) % 4
        for near in (g, after):
            if (l, near, "halo") not in ready:
                ready.add((l, near, "halo"))
                for k in range(2):
                    halo(l, near, k).wait_recv()
        for c in range(2):
            lo = c * CH
            q = jnp.concatenate(
                [qs[g, TILE // 2 :, lo : lo + CH], qs[after, : TILE // 2, lo : lo + CH]], axis=0
            )
            q_all = jnp.concatenate([q * m for m in head_mask], axis=0)
            table = bias[l, 4 * c : 4 * c + 4].reshape(4 * TILE, 3 * 128)
            scores = jnp.concatenate(
                [dot_nt(q_all, window(l, j, g, lo)) for j in range(3)], axis=1
            ) + table
            highest = jnp.max(scores, axis=1, keepdims=True)
            weights = jnp.exp(scores - highest)
            total = jnp.sum(weights, axis=1, keepdims=True)
            weights = weights.astype(BF16)
            values = jnp.concatenate([window(l, j, g, PAIR + lo) for j in range(3)], axis=0)
            o = dot(weights, values) / total
            out = o[:TILE]
            for h in range(1, 4):
                out = jnp.where(lane_head == h, o[h * TILE : (h + 1) * TILE], out)
            mixed[g, :, lo : lo + CH] = out.astype(BF16)
        if l < LAYERS - 1 and (l, "across") not in ready:
            ready.add((l, "across"))
            for i in range(parts):
                weights_across(l + 1, i).start()

    def chunk(l, g, k):
        piece = dot(mixed[g], wout[l, sides[k]])
        return piece[:, :CH], piece[:, CH:]

    def step_first(l, g):
        weights_in(l, 1, range(3, parts))
        for half, piece in enumerate(chunk(l, g, 0)):
            ssum[g, 0, half] = piece.astype(BF16)
        ring(g, 0).start()
        ring(g, 1).start()

    def step_rest(l, g):
        for k in (1, 2):
            for half, piece in enumerate(chunk(l, g, k)):
                ssum[g, k, half] = piece.astype(BF16)
        ring(g, 2).start()
        ring(g, 3).start()
        after = (g + 1) % 4
        for half, piece in enumerate(chunk(l, g, 3)):
            before = jnp.concatenate(
                [xg[l, g, y, half, TILE // 2 :], xg[l, after, y, half, : TILE // 2]], axis=0
            )
            own[g, half] = piece + before.astype(F32)

    def step_add(l, g):
        for k in range(2):
            ring(g, k).wait_recv()
            side = 1 + k
            ssum[g, side, k] = (ssum[g, side, k].astype(F32) + rs_y[g, k].astype(F32)).astype(BF16)
            ring(g, 4 + k).start()

    def step_finish(l, g):
        for k in (2, 3, 4, 5):
            ring(g, k).wait_recv()
        new = (
            own[g, 0] + rs_y[g, 4].astype(F32) + rs_y[g, 3].astype(F32),
            own[g, 1] + rs_y[g, 2].astype(F32) + rs_y[g, 5].astype(F32),
        )
        if l < LAYERS - 1:
            for half in range(2):
                xg[l + 1, g, y, half] = new[half].astype(BF16)
            step_own(l + 1, g)
        else:
            for half in range(2):
                o_src[half, 8 * g : 8 * g + 8] = new[half].reshape(8, STRIP_C, CH).astype(BF16)

            def send(r, carry):
                slot = 8 * g + r
                row = (slot + LAYERS * WIN_R // 2) % ROWS
                there, spot = row // rows, row % rows

                @pl.when(there != sp)
                def _():
                    remote(
                        o_src.at[core, slot], o_dst.at[core, sp, spot], o_s.at[0], o_r.at[core],
                        {"sp": there},
                    ).start()

                @pl.when(there == sp)
                def _():
                    o_dst[core, sp, spot] = o_src[core, slot]

                remote(
                    o_src.at[1 - core, slot], o_dst.at[core, sp, spot], o_s.at[1], o_r.at[core],
                    {"sp": there, "tp": partner},
                ).start()
                return carry

            lax.fori_loop(0, 8, send, 0)
        for k in range(6):
            ring(g, k).wait_send()

    steps = (
        step_own, step_relay, step_mine, step_sides, step_far,
        step_attend, step_first, step_rest, step_add, step_finish,
    )
    for step, l, g in ORDER:
        steps[step](l, g)

    for l in range(LAYERS):
        for i in range(parts):
            weights_across(l, i).wait_send()
    for l in range(LAYERS):
        for g in range(GROUPS):
            for k in range(2):
                halo(l, g, k).wait_send()
    gone = x_src.at[pl.ds(0, n_sp - 1), core]
    pltpu.make_async_copy(gone, gone, x_s.at[0]).wait()
    gone = x_src.at[:, core]
    pltpu.make_async_copy(gone, gone, x_s.at[1]).wait()
    gone = o_src.at[core, pl.ds(0, ROWS - rows)]
    pltpu.make_async_copy(gone, gone, o_s.at[0]).wait()
    gone = o_src.at[1 - core]
    pltpu.make_async_copy(gone, gone, o_s.at[1]).wait()
    most = o_dst.at[core, pl.ds(0, n_sp - 1)]
    pltpu.make_async_copy(most, most, o_r.at[core]).wait()
    rest = o_dst.at[1 - core]
    pltpu.make_async_copy(rest, rest, o_r.at[1 - core]).wait()
    for r in range(rows):
        both = jnp.stack([o_dst[c, :, r].astype(F32) for c in range(2)], axis=1)
        out_ref[r] = both.reshape(n_sp * WIN_C, CH).T.astype(BF16)


def body(token_grid, norm_gain, w_query, w_key, w_value, w_out, rel_bias):
    n_sp = lax.axis_size("sp")
    rows = token_grid.shape[0]
    wq, wk, wv = (w.reshape(LAYERS, N_TP, CH, CH) for w in (w_query, w_key, w_value))
    vmem = pl.BlockSpec(memory_space=pltpu.VMEM)
    hbm = pl.BlockSpec(memory_space=pl.ANY)
    dma = pltpu.SemaphoreType.DMA
    parts = 3 + CHIPS
    return pl.pallas_call(
        functools.partial(kernel, n_sp, rows),
        out_shape=jax.ShapeDtypeStruct(token_grid.shape, BF16),
        in_specs=[vmem, vmem, vmem, hbm, hbm, hbm, hbm],
        out_specs=vmem,
        scratch_shapes=[
            pltpu.VMEM((n_sp, 2, rows, STRIP_C, CH), BF16),
            pltpu.VMEM((2, ROWS, STRIP_C, CH), BF16),
            pltpu.VMEM((2, ROWS, STRIP_C, CH), BF16),
            pltpu.VMEM((2, n_sp, rows, STRIP_C, CH), BF16),
            pltpu.VMEM((LAYERS, N_TP, CH, 3 * PAIR), BF16),
            pltpu.VMEM((LAYERS, CHIPS, PAIR, PAIR), BF16),
            pltpu.VMEM((LAYERS, N_TP, 1, CH), F32),
            pltpu.VMEM((2, LAYERS, 4, WIN_R, WIN_C), F32),
            pltpu.VMEM((LAYERS, HEADS, WIN_R, 128), F32),
            pltpu.VMEM((LAYERS, HEADS, TILE, 3 * 128), F32),
            pltpu.VMEM((LAYERS, GROUPS, CHIPS, 2, TILE, CH), BF16),
            pltpu.VMEM((GROUPS, TILE, 3 * PAIR), F32),
            pltpu.VMEM((GROUPS, TILE, 128), F32),
            pltpu.VMEM((GROUPS, TILE, PAIR), BF16),
            pltpu.VMEM((LAYERS, 3, GROUPS, TILE, 2 * PAIR), BF16),
            pltpu.VMEM((GROUPS, TILE, PAIR), BF16),
            pltpu.VMEM((GROUPS, 3, 2, TILE, CH), BF16),
            pltpu.VMEM((GROUPS, 2, TILE, CH), F32),
            pltpu.VMEM((GROUPS, 6, TILE, CH), BF16),
            dma((LAYERS, parts)), dma((LAYERS, parts)), dma((LAYERS, parts)),
            dma((1,)), dma((1,)), dma((2,)), dma((2,)), dma((2,)), dma((2,)),
            dma((GROUPS, 6)), dma((GROUPS, 6)), dma((GROUPS, 6)), dma((GROUPS, 6)),
            dma((LAYERS, GROUPS, 2)), dma((LAYERS, GROUPS, 2)),
        ],
        compiler_params=pltpu.CompilerParams(
            collective_id=0, has_side_effects=True, vmem_limit_bytes=60 * 1024 * 1024
        ),
    )(token_grid, norm_gain, rel_bias, wq, wk, wv, w_out)


def solution(mesh):
    in_specs = (
        P("sp", "tp", None),
        P(),
        P(None, None, "tp"),
        P(None, None, "tp"),
        P(None, None, "tp"),
        P(None, "tp", None),
        P(None, "tp", None, None),
    )
    out_specs = P("sp", "tp", None)
    return jax.shard_map(body, mesh=mesh, in_specs=in_specs, out_specs=out_specs, check_vma=False)
```

```python
import functools

import jax
import jax.numpy as jnp
from jax import lax
from jax.experimental import pallas as pl
from jax.experimental.pallas import tpu as pltpu
from jax.sharding import PartitionSpec as P

D = 2048
HEAD_DIM = 64
CH = 256
PAIR = 2 * CH
N_TP = 8
CHIPS = 4
WIN_R = 8
WIN_C = 16
LAYERS = 3
HEADS = 8
ROWS = 32
GROUPS = 4
STRIP_C = 8
TILE = 64
EPS = 1e-06
NEG = -1e30
MESH = pl.DeviceIdType.MESH
F32 = jnp.float32
BF16 = jnp.bfloat16

OWN, RELAY, MINE, SIDES, FAR, ATTEND, FIRST, REST, ADD, FINISH = range(10)
ORDER = (
    (OWN, 0, 2), (OWN, 0, 3), (OWN, 0, 0), (OWN, 0, 1), (MINE, 0, 2),
    (MINE, 0, 3), (MINE, 0, 0), (RELAY, 0, 2), (SIDES, 0, 2), (RELAY, 0, 3),
    (SIDES, 0, 3), (RELAY, 0, 0), (SIDES, 0, 0), (RELAY, 0, 1), (MINE, 0, 1),
    (SIDES, 0, 1), (FAR, 0, 2), (FAR, 0, 3), (FAR, 0, 0), (FAR, 0, 1),
    (ATTEND, 0, 2), (FIRST, 0, 2), (REST, 0, 2), (ATTEND, 0, 3), (FIRST, 0, 3),
    (REST, 0, 3), (ATTEND, 0, 0), (FIRST, 0, 0), (ADD, 0, 2), (REST, 0, 0),
    (ATTEND, 0, 1), (FIRST, 0, 1), (ADD, 0, 3), (REST, 0, 1), (ADD, 0, 0),
    (FINISH, 0, 2), (MINE, 1, 2), (ADD, 0, 1), (FINISH, 0, 3), (MINE, 1, 3),
    (RELAY, 1, 2), (FINISH, 0, 0), (MINE, 1, 0), (SIDES, 1, 2), (RELAY, 1, 3),
    (FINISH, 0, 1), (SIDES, 1, 3), (FAR, 1, 2), (RELAY, 1, 0), (SIDES, 1, 0),
    (FAR, 1, 3), (RELAY, 1, 1), (FAR, 1, 0), (MINE, 1, 1), (SIDES, 1, 1),
    (FAR, 1, 1), (ATTEND, 1, 2), (FIRST, 1, 2), (REST, 1, 2), (ATTEND, 1, 3),
    (FIRST, 1, 3), (REST, 1, 3), (ADD, 1, 2), (ATTEND, 1, 0), (FIRST, 1, 0),
    (REST, 1, 0), (ADD, 1, 3), (ATTEND, 1, 1), (FIRST, 1, 1), (FINISH, 1, 2),
    (MINE, 2, 2), (ADD, 1, 0), (REST, 1, 1), (FINISH, 1, 3), (ADD, 1, 1),
    (MINE, 2, 3), (RELAY, 2, 2), (FINISH, 1, 0), (MINE, 2, 0), (SIDES, 2, 2),
    (RELAY, 2, 3), (FINISH, 1, 1), (MINE, 2, 1), (FAR, 2, 2), (RELAY, 2, 0),
    (SIDES, 2, 3), (SIDES, 2, 0), (RELAY, 2, 1), (FAR, 2, 3), (SIDES, 2, 1),
    (FAR, 2, 0), (FAR, 2, 1), (ATTEND, 2, 2), (FIRST, 2, 2), (REST, 2, 2),
    (ATTEND, 2, 3), (FIRST, 2, 3), (REST, 2, 3), (ATTEND, 2, 0), (FIRST, 2, 0),
    (REST, 2, 0), (ATTEND, 2, 1), (FIRST, 2, 1), (REST, 2, 1), (ADD, 2, 2),
    (ADD, 2, 3), (ADD, 2, 0), (ADD, 2, 1), (FINISH, 2, 2), (FINISH, 2, 3),
    (FINISH, 2, 0), (FINISH, 2, 1),
)


def dot(a, b):
    return lax.dot_general(a, b, (((1,), (0,)), ((), ())), preferred_element_type=F32)


def dot_nt(a, b):
    return lax.dot_general(a, b, (((1,), (1,)), ((), ())), preferred_element_type=F32)


def kernel(
    n_sp, rows, x_ref, gain_ref, bias_ref, wq_ref, wk_ref, wv_ref, wo_ref, out_ref,
    x_src, x_dst, o_src, o_dst, wqkv, wout, gains, heads, pad, bias,
    xg, acc, sq, qs, kv, mixed, ssum, own, rs_y,
    w_sem, wr_s, wr_r, b_s, b_r, x_s, x_r, o_s, o_r, ag_s, ag_r, y_s, y_r, h_s, h_r,
):
    tp = lax.axis_index("tp")
    sp = lax.axis_index("sp")
    y, core = tp // 2, tp % 2
    right, left, opp = (y + 1) % 4, (y + 3) % 4, (y + 2) % 4
    partner = y * 2 + 1 - core

    barrier = pltpu.get_barrier_semaphore()
    for target in (right * 2 + core, left * 2 + core, partner):
        pl.semaphore_signal(barrier, inc=1, device_id={"tp": target}, device_id_type=MESH)

    def greet(i, carry):
        there = (sp + i) % n_sp
        pl.semaphore_signal(barrier, inc=1, device_id={"sp": there}, device_id_type=MESH)
        pl.semaphore_signal(
            barrier, inc=1, device_id={"sp": there, "tp": partner}, device_id_type=MESH
        )
        return carry

    lax.fori_loop(1, n_sp, greet, 0)

    def remote(src, dst, s_sem, r_sem, target):
        return pltpu.make_async_remote_copy(
            src_ref=src, dst_ref=dst, send_sem=s_sem, recv_sem=r_sem,
            device_id=target, device_id_type=MESH,
        )

    def weight_pairs(l):
        pairs = []
        for i, ref in enumerate((wq_ref, wk_ref, wv_ref)):
            lanes = pl.ds(pl.multiple_of(i * PAIR + core * CH, CH), CH)
            pairs.append((ref.at[l], wqkv.at[l, :, :, lanes]))
        for b in range(CHIPS):
            pairs.append(
                (wo_ref.at[l, :, pl.ds(b * PAIR, PAIR)], wout.at[l, b, pl.ds(core * CH, CH)])
            )
        return pairs

    def weights_here(l, i):
        src, dst = weight_pairs(l)[i]
        return pltpu.make_async_copy(src, dst, w_sem.at[l, i])

    def weights_across(l, i):
        src, dst = weight_pairs(l)[i]
        return remote(src, dst, wr_s.at[l, i], wr_r.at[l, i], {"tp": partner})

    parts = 3 + CHIPS
    for l in range(LAYERS):
        for i in range(parts):
            weights_here(l, i).start()

    for r in range(rows):
        turned = x_ref[r].astype(F32).T.reshape(n_sp, 2, STRIP_C, CH).astype(BF16)
        for c in range(2):
            x_src[:, c, r] = turned[:, c]

    here = pl.ds(sp * rows, rows)

    def scatter_in(i, carry):
        there = (sp + i) % n_sp

        @pl.when(i > 0)
        def _():
            remote(
                x_src.at[there, core], x_dst.at[core, here], x_s.at[0], x_r.at[core], {"sp": there}
            ).start()

        remote(
            x_src.at[there, 1 - core], x_dst.at[core, here], x_s.at[1], x_r.at[core],
            {"sp": there, "tp": partner},
        ).start()
        return carry

    pl.semaphore_wait(barrier, 2 * n_sp + 1)
    lax.fori_loop(0, n_sp, scatter_in, 0)
    bias_copy = remote(bias_ref, heads.at[core], b_s.at[0], b_r.at[0], {"tp": partner})
    bias_copy.start()
    for i in range(parts):
        weights_across(0, i).start()
    x_dst[core, here] = x_src[sp, core]
    heads[core] = bias_ref[...]

    for l in range(LAYERS):
        for b in range(N_TP):
            gains[l, b] = gain_ref[l : l + 1, b * CH : (b + 1) * CH].astype(F32)
    pad[...] = jnp.zeros_like(pad)
    bias_copy.wait()
    for l in range(LAYERS):
        for h in range(HEADS):
            pad[l, h, :, :WIN_C] = heads[h // 4, l, h % 4]
    lane = lax.broadcasted_iota(jnp.int32, (8, 128), 1)
    lane_c = lane % STRIP_C
    row_c = lax.broadcasted_iota(jnp.int32, (8, 128), 0)
    nothing = jnp.full((8, 128), NEG, F32)

    def build(l, carry):
        for h in range(HEADS):
            table = pad[l, h]
            lanes = []
            for j in range(2):
                piece = table if j == 0 else pltpu.roll(table, 128 - STRIP_C, 1)
                piece = jnp.where(lane < STRIP_C, piece, 0.0)
                piece = pltpu.roll(piece, 0, 1, stride=STRIP_C, stride_axis=0)
                piece = jnp.broadcast_to(jnp.sum(piece, axis=0, keepdims=True), (8, 128))
                lanes.append(jnp.where(lane < WIN_R * STRIP_C, piece, NEG))
            straight = [pltpu.roll(g, 0, 1, stride=1, stride_axis=0) for g in lanes] + [nothing]
            carried = [nothing] + [
                pltpu.roll(g, 128 - STRIP_C, 1, stride=1, stride_axis=0) for g in lanes
            ]
            for j in range(3):
                t = jnp.where(lane_c >= row_c, straight[j], carried[j])
                for r in range(8):
                    bias[l, h, r * 8 : (r + 1) * 8, j * 128 : (j + 1) * 128] = (
                        t if r == 0 else pltpu.roll(t, r * STRIP_C, 1)
                    )
        return carry

    lax.fori_loop(0, LAYERS, build, 0)

    most = x_dst.at[core, pl.ds(0, ROWS - rows)]
    pltpu.make_async_copy(most, most, x_r.at[core]).wait()
    rest = x_dst.at[1 - core]
    pltpu.make_async_copy(rest, rest, x_r.at[1 - core]).wait()
    for g in range(GROUPS):
        for h in range(2):
            xg[0, g, y, h] = (
                x_dst[h, g * 8 : (g + 1) * 8].astype(F32).reshape(TILE, CH).astype(BF16)
            )

    to_right, to_left = right * 2 + core, left * 2 + core
    gather = (
        (y, 0, to_right), (y, 1, to_right), (left, 0, to_right),
        (y, 1, to_left), (y, 0, to_left), (right, 1, to_left),
    )

    def ag(l, g, k):
        owner, half, target = gather[k]
        ref = xg.at[l, g, owner, half]
        return remote(ref, ref, ag_s.at[g, k], ag_r.at[g, k], {"tp": target})

    sides = (opp, right, left, y)
    scatter = (
        (0, 0, to_right), (0, 1, to_left), (1, 1, to_right),
        (2, 0, to_left), (1, 0, to_right), (2, 1, to_left),
    )

    def ring(g, k):
        side, half, target = scatter[k]
        return remote(
            ssum.at[g, side, half], rs_y.at[g, k], y_s.at[g, k], y_r.at[g, k], {"tp": target}
        )

    def halo(l, g, k):
        slot = 2 * core if k else 2 * (1 - core)
        target = {"tp": partner}
        if k == 0:
            target["sp"] = (sp + 2 * core - 1 + n_sp) % n_sp
        return remote(kv.at[l, 1, g], kv.at[l, slot, g], h_s.at[l, g, k], h_r.at[l, g, k], target)

    lane_head = lax.broadcasted_iota(jnp.int32, (TILE, CH), 1) // HEAD_DIM
    ones = jnp.ones((3 * 128, 128), BF16)
    head_mask = [(lane_head == h).astype(F32).astype(BF16) for h in range(4)]

    def step_own(l, g):
        for k in (0, 3, 1, 4):
            ag(l, g, k).start()

    def step_relay(l, g):
        for k, onward in ((0, 2), (3, 5)):
            ag(l, g, k).wait_recv()
            ag(l, g, onward).start()

    def accumulate(l, g, blocks, fresh):
        total = None
        squares = None
        for chip, half in blocks:
            wide = xg[l, g, chip, half].astype(F32)
            sq_b = wide * wide
            sq_b = sq_b[:, :128] + sq_b[:, 128:]
            squares = sq_b if squares is None else squares + sq_b
            b = chip * 2 + half
            term = dot((wide * gains[l, b]).astype(BF16), wqkv[l, b])
            total = term if total is None else total + term
        if fresh:
            acc[g] = total
            sq[g] = squares
        else:
            acc[g] += total
            sq[g] += squares

    ready = set()

    def weights_in(l, which, parts_of):
        if (l, which) in ready:
            return
        ready.add((l, which))
        for i in parts_of:
            weights_here(l, i).wait()
            weights_across(l, i).wait_recv()

    def step_mine(l, g):
        weights_in(l, 0, range(3))
        accumulate(l, g, ((y, 0), (y, 1)), True)

    def step_sides(l, g):
        ag(l, g, 1).wait_recv()
        ag(l, g, 4).wait_recv()
        accumulate(l, g, ((left, 0), (right, 1), (left, 1), (right, 0)), False)

    def step_far(l, g):
        ag(l, g, 2).wait_recv()
        ag(l, g, 5).wait_recv()
        squares = sq[g]
        scaled = []
        for half in range(2):
            wide = xg[l, g, opp, half].astype(F32)
            scaled.append((wide * gains[l, opp * 2 + half]).astype(BF16))
            wide = wide * wide
            squares = squares + wide[:, :128] + wide[:, 128:]
        inverse = lax.rsqrt(jnp.sum(squares, axis=1, keepdims=True) / D + EPS)

        def total(lo, hi):
            return acc[g, :, lo:hi] + (
                dot(scaled[0], wqkv[l, opp * 2, :, lo:hi])
                + dot(scaled[1], wqkv[l, opp * 2 + 1, :, lo:hi])
            )

        kv[l, 1, g] = (total(PAIR, 3 * PAIR) * inverse).astype(BF16)
        for k in range(2):
            halo(l, g, k).start()
        qs[g] = (total(0, PAIR) * (inverse * HEAD_DIM**-0.5)).astype(BF16)
        for k in range(6):
            ag(l, g, k).wait_send()

    def window(l, slot, g, lo):
        return jnp.concatenate(
            [kv[l, slot, g, :, lo : lo + CH], kv[l, slot, (g + 1) % 4, :, lo : lo + CH]], axis=0
        )

    def step_attend(l, g):
        after = (g + 1) % 4
        for near in (g, after):
            if (l, near, "halo") not in ready:
                ready.add((l, near, "halo"))
                for k in range(2):
                    halo(l, near, k).wait_recv()
        scores, values = [], []
        for c in range(2):
            lo = c * CH
            q = jnp.concatenate(
                [qs[g, TILE // 2 :, lo : lo + CH], qs[after, : TILE // 2, lo : lo + CH]], axis=0
            )
            q_all = jnp.concatenate([q * m for m in head_mask], axis=0)
            table = bias[l, 4 * c : 4 * c + 4].reshape(4 * TILE, 3 * 128)
            scores.append(
                [dot_nt(q_all, window(l, j, g, lo)) + table[:, j * 128 : (j + 1) * 128] for j in range(3)]
            )
            values.append([window(l, j, g, PAIR + lo) for j in range(3)])
        highest = [
            jnp.max(jnp.maximum(jnp.maximum(s[0], s[1]), s[2]), axis=1, keepdims=True) for s in scores
        ]
        weights = [[jnp.exp(s - top).astype(BF16) for s in ss] for ss, top in zip(scores, highest)]
        for c in range(2):
            wide = jnp.concatenate(weights[c], axis=1)
            total = dot(wide, ones)
            o = dot(wide, jnp.concatenate(values[c], axis=0))
            o = o * (1.0 / jnp.concatenate([total, total], axis=1))
            out = o[:TILE]
            for h in range(1, 4):
                out = jnp.where(lane_head == h, o[h * TILE : (h + 1) * TILE], out)
            mixed[g, :, c * CH : (c + 1) * CH] = out.astype(BF16)
        if l < LAYERS - 1 and (l, "across") not in ready:
            ready.add((l, "across"))
            for i in range(parts):
                weights_across(l + 1, i).start()

    def chunk(l, g, k):
        piece = dot(mixed[g], wout[l, sides[k]])
        return piece[:, :CH], piece[:, CH:]

    def step_first(l, g):
        weights_in(l, 1, range(3, parts))
        for half, piece in enumerate(chunk(l, g, 0)):
            ssum[g, 0, half] = piece.astype(BF16)
        ring(g, 0).start()
        ring(g, 1).start()

    def step_rest(l, g):
        for k in (1, 2):
            for half, piece in enumerate(chunk(l, g, k)):
                ssum[g, k, half] = piece.astype(BF16)
        ring(g, 2).start()
        ring(g, 3).start()
        after = (g + 1) % 4
        for half, piece in enumerate(chunk(l, g, 3)):
            before = jnp.concatenate(
                [xg[l, g, y, half, TILE // 2 :], xg[l, after, y, half, : TILE // 2]], axis=0
            )
            own[g, half] = piece + before.astype(F32)

    def step_add(l, g):
        for k in range(2):
            ring(g, k).wait_recv()
            side = 1 + k
            ssum[g, side, k] = (ssum[g, side, k].astype(F32) + rs_y[g, k].astype(F32)).astype(BF16)
            ring(g, 4 + k).start()

    def step_finish(l, g):
        for k in (2, 3, 4, 5):
            ring(g, k).wait_recv()
        new = (
            own[g, 0] + rs_y[g, 4].astype(F32) + rs_y[g, 3].astype(F32),
            own[g, 1] + rs_y[g, 2].astype(F32) + rs_y[g, 5].astype(F32),
        )
        if l < LAYERS - 1:
            for half in range(2):
                xg[l + 1, g, y, half] = new[half].astype(BF16)
            step_own(l + 1, g)
        else:
            for half in range(2):
                o_src[half, 8 * g : 8 * g + 8] = new[half].reshape(8, STRIP_C, CH).astype(BF16)

            def send(r, carry):
                slot = 8 * g + r
                row = (slot + LAYERS * WIN_R // 2) % ROWS
                there, spot = row // rows, row % rows

                @pl.when(there != sp)
                def _():
                    remote(
                        o_src.at[core, slot], o_dst.at[core, sp, spot], o_s.at[0], o_r.at[core],
                        {"sp": there},
                    ).start()

                @pl.when(there == sp)
                def _():
                    o_dst[core, sp, spot] = o_src[core, slot]

                remote(
                    o_src.at[1 - core, slot], o_dst.at[core, sp, spot], o_s.at[1], o_r.at[core],
                    {"sp": there, "tp": partner},
                ).start()
                return carry

            lax.fori_loop(0, 8, send, 0)
        for k in range(6):
            ring(g, k).wait_send()

    steps = (
        step_own, step_relay, step_mine, step_sides, step_far,
        step_attend, step_first, step_rest, step_add, step_finish,
    )
    for step, l, g in ORDER:
        steps[step](l, g)

    for l in range(LAYERS):
        for i in range(parts):
            weights_across(l, i).wait_send()
    for l in range(LAYERS):
        for g in range(GROUPS):
            for k in range(2):
                halo(l, g, k).wait_send()
    gone = x_src.at[pl.ds(0, n_sp - 1), core]
    pltpu.make_async_copy(gone, gone, x_s.at[0]).wait()
    gone = x_src.at[:, core]
    pltpu.make_async_copy(gone, gone, x_s.at[1]).wait()
    gone = o_src.at[core, pl.ds(0, ROWS - rows)]
    pltpu.make_async_copy(gone, gone, o_s.at[0]).wait()
    gone = o_src.at[1 - core]
    pltpu.make_async_copy(gone, gone, o_s.at[1]).wait()
    most = o_dst.at[core, pl.ds(0, n_sp - 1)]
    pltpu.make_async_copy(most, most, o_r.at[core]).wait()
    rest = o_dst.at[1 - core]
    pltpu.make_async_copy(rest, rest, o_r.at[1 - core]).wait()
    for r in range(rows):
        both = jnp.stack([o_dst[c, :, r].astype(F32) for c in range(2)], axis=1)
        out_ref[r] = both.reshape(n_sp * WIN_C, CH).T.astype(BF16)


def body(token_grid, norm_gain, w_query, w_key, w_value, w_out, rel_bias):
    n_sp = lax.axis_size("sp")
    rows = token_grid.shape[0]
    wq, wk, wv = (w.reshape(LAYERS, N_TP, CH, CH) for w in (w_query, w_key, w_value))
    vmem = pl.BlockSpec(memory_space=pltpu.VMEM)
    hbm = pl.BlockSpec(memory_space=pltpu.HBM)
    dma = pltpu.SemaphoreType.DMA
    parts = 3 + CHIPS
    return pl.pallas_call(
        functools.partial(kernel, n_sp, rows),
        out_shape=jax.ShapeDtypeStruct(token_grid.shape, BF16),
        in_specs=[vmem, vmem, vmem, hbm, hbm, hbm, hbm],
        out_specs=vmem,
        scratch_shapes=[
            pltpu.VMEM((n_sp, 2, rows, STRIP_C, CH), BF16),
            pltpu.VMEM((2, ROWS, STRIP_C, CH), BF16),
            pltpu.VMEM((2, ROWS, STRIP_C, CH), BF16),
            pltpu.VMEM((2, n_sp, rows, STRIP_C, CH), BF16),
            pltpu.VMEM((LAYERS, N_TP, CH, 3 * PAIR), BF16),
            pltpu.VMEM((LAYERS, CHIPS, PAIR, PAIR), BF16),
            pltpu.VMEM((LAYERS, N_TP, 1, CH), F32),
            pltpu.VMEM((2, LAYERS, 4, WIN_R, WIN_C), F32),
            pltpu.VMEM((LAYERS, HEADS, WIN_R, 128), F32),
            pltpu.VMEM((LAYERS, HEADS, TILE, 3 * 128), F32),
            pltpu.VMEM((LAYERS, GROUPS, CHIPS, 2, TILE, CH), BF16),
            pltpu.VMEM((GROUPS, TILE, 3 * PAIR), F32),
            pltpu.VMEM((GROUPS, TILE, 128), F32),
            pltpu.VMEM((GROUPS, TILE, PAIR), BF16),
            pltpu.VMEM((LAYERS, 3, GROUPS, TILE, 2 * PAIR), BF16),
            pltpu.VMEM((GROUPS, TILE, PAIR), BF16),
            pltpu.VMEM((GROUPS, 3, 2, TILE, CH), BF16),
            pltpu.VMEM((GROUPS, 2, TILE, CH), F32),
            pltpu.VMEM((GROUPS, 6, TILE, CH), BF16),
            dma((LAYERS, parts)), dma((LAYERS, parts)), dma((LAYERS, parts)),
            dma((1,)), dma((1,)), dma((2,)), dma((2,)), dma((2,)), dma((2,)),
            dma((GROUPS, 6)), dma((GROUPS, 6)), dma((GROUPS, 6)), dma((GROUPS, 6)),
            dma((LAYERS, GROUPS, 2)), dma((LAYERS, GROUPS, 2)),
        ],
        compiler_params=pltpu.CompilerParams(
            collective_id=0, has_side_effects=True, vmem_limit_bytes=52 * 1024 * 1024
        ),
    )(token_grid, norm_gain, rel_bias, wq, wk, wv, w_out)


def solution(mesh):
    in_specs = (
        P("sp", "tp", None),
        P(),
        P(None, None, "tp"),
        P(None, None, "tp"),
        P(None, None, "tp"),
        P(None, "tp", None),
        P(None, "tp", None, None),
    )
    out_specs = P("sp", "tp", None)
    return jax.shard_map(body, mesh=mesh, in_specs=in_specs, out_specs=out_specs, check_vma=False)
```

```python
import functools

import jax
import jax.numpy as jnp
from jax import lax
from jax.experimental import pallas as pl
from jax.experimental.pallas import tpu as pltpu
from jax.sharding import PartitionSpec as P

D = 2048
HEAD_DIM = 64
CH = 256
PAIR = 2 * CH
N_TP = 8
CHIPS = 4
WIN_R = 8
WIN_C = 16
LAYERS = 3
HEADS = 8
ROWS = 32
GROUPS = 4
STRIP_C = 8
TILE = 64
EPS = 1e-06
NEG = -1e30
MESH = pl.DeviceIdType.MESH
F32 = jnp.float32
BF16 = jnp.bfloat16

OWN, RELAY, MINE, SIDES, FAR, ATTEND, FIRST, REST, ADD, FINISH = range(10)
ORDER = (
    (OWN, 0, 0), (OWN, 0, 3), (MINE, 0, 0), (MINE, 0, 3), (OWN, 0, 1),
    (OWN, 0, 2), (MINE, 0, 1), (MINE, 0, 2), (RELAY, 0, 0), (SIDES, 0, 0),
    (RELAY, 0, 3), (SIDES, 0, 3), (RELAY, 0, 1), (SIDES, 0, 1), (RELAY, 0, 2),
    (SIDES, 0, 2), (FAR, 0, 0), (FAR, 0, 3), (FAR, 0, 1), (FAR, 0, 2),
    (ATTEND, 0, 3), (FIRST, 0, 3), (REST, 0, 3), (ATTEND, 0, 0), (FIRST, 0, 0),
    (REST, 0, 0), (ATTEND, 0, 1), (FIRST, 0, 1), (REST, 0, 1), (ADD, 0, 3),
    (ATTEND, 0, 2), (FIRST, 0, 2), (ADD, 0, 0), (REST, 0, 2), (ADD, 0, 1),
    (FINISH, 0, 3), (MINE, 1, 3), (ADD, 0, 2), (FINISH, 0, 0), (MINE, 1, 0),
    (FINISH, 0, 1), (MINE, 1, 1), (RELAY, 1, 3), (SIDES, 1, 3), (FINISH, 0, 2),
    (MINE, 1, 2), (RELAY, 1, 0), (SIDES, 1, 0), (RELAY, 1, 1), (SIDES, 1, 1),
    (FAR, 1, 3), (RELAY, 1, 2), (SIDES, 1, 2), (FAR, 1, 0), (FAR, 1, 1),
    (FAR, 1, 2), (ATTEND, 1, 3), (FIRST, 1, 3), (REST, 1, 3), (ATTEND, 1, 0),
    (FIRST, 1, 0), (REST, 1, 0), (ATTEND, 1, 2), (FIRST, 1, 2), (REST, 1, 2),
    (ADD, 1, 3), (ATTEND, 1, 1), (FIRST, 1, 1), (ADD, 1, 0), (REST, 1, 1),
    (ADD, 1, 2), (FINISH, 1, 3), (MINE, 2, 3), (ADD, 1, 1), (FINISH, 1, 0),
    (MINE, 2, 0), (FINISH, 1, 2), (MINE, 2, 2), (RELAY, 2, 3), (SIDES, 2, 3),
    (FINISH, 1, 1), (MINE, 2, 1), (RELAY, 2, 0), (SIDES, 2, 0), (RELAY, 2, 2),
    (SIDES, 2, 2), (FAR, 2, 3), (RELAY, 2, 1), (SIDES, 2, 1), (FAR, 2, 0),
    (FAR, 2, 2), (FAR, 2, 1), (ATTEND, 2, 3), (FIRST, 2, 3), (REST, 2, 3),
    (ATTEND, 2, 2), (FIRST, 2, 2), (REST, 2, 2), (ATTEND, 2, 0), (FIRST, 2, 0),
    (REST, 2, 0), (ATTEND, 2, 1), (FIRST, 2, 1), (REST, 2, 1), (ADD, 2, 2),
    (ADD, 2, 3), (ADD, 2, 0), (ADD, 2, 1), (FINISH, 2, 2), (FINISH, 2, 3),
    (FINISH, 2, 0), (FINISH, 2, 1),
)


def dot(a, b):
    return lax.dot_general(a, b, (((1,), (0,)), ((), ())), preferred_element_type=F32)


def dot_nt(a, b):
    return lax.dot_general(a, b, (((1,), (1,)), ((), ())), preferred_element_type=F32)


def kernel(
    n_sp, rows, x_ref, gain_ref, bias_ref, wq_ref, wk_ref, wv_ref, wo_ref, out_ref,
    x_src, x_dst, o_src, o_dst, wqkv, wout, gains, heads, pad, bias,
    xg, acc, sq, qs, kv, mixed, ssum, own, rs_y,
    w_sem, wr_s, wr_r, b_s, b_r, x_s, x_r, o_s, o_r, ag_s, ag_r, y_s, y_r, h_s, h_r,
):
    tp = lax.axis_index("tp")
    sp = lax.axis_index("sp")
    y, core = tp // 2, tp % 2
    right, left, opp = (y + 1) % 4, (y + 3) % 4, (y + 2) % 4
    partner = y * 2 + 1 - core

    barrier = pltpu.get_barrier_semaphore()
    for target in (right * 2 + core, left * 2 + core, partner):
        pl.semaphore_signal(barrier, inc=1, device_id={"tp": target}, device_id_type=MESH)

    def greet(i, carry):
        there = (sp + i) % n_sp
        pl.semaphore_signal(barrier, inc=1, device_id={"sp": there}, device_id_type=MESH)
        pl.semaphore_signal(
            barrier, inc=1, device_id={"sp": there, "tp": partner}, device_id_type=MESH
        )
        return carry

    lax.fori_loop(1, n_sp, greet, 0)

    def remote(src, dst, s_sem, r_sem, target):
        return pltpu.make_async_remote_copy(
            src_ref=src, dst_ref=dst, send_sem=s_sem, recv_sem=r_sem,
            device_id=target, device_id_type=MESH,
        )

    def weight_pairs(l):
        pairs = []
        for i, ref in enumerate((wq_ref, wk_ref, wv_ref)):
            lanes = pl.ds(pl.multiple_of(i * PAIR + core * CH, CH), CH)
            pairs.append((ref.at[l], wqkv.at[l, :, :, lanes]))
        for b in range(CHIPS):
            pairs.append(
                (wo_ref.at[l, :, pl.ds(b * PAIR, PAIR)], wout.at[l, b, pl.ds(core * CH, CH)])
            )
        return pairs

    def weights_here(l, i):
        src, dst = weight_pairs(l)[i]
        return pltpu.make_async_copy(src, dst, w_sem.at[l, i])

    def weights_across(l, i):
        src, dst = weight_pairs(l)[i]
        return remote(src, dst, wr_s.at[l, i], wr_r.at[l, i], {"tp": partner})

    parts = 3 + CHIPS
    for l in range(LAYERS):
        for i in range(parts):
            weights_here(l, i).start()

    for r in range(rows):
        turned = x_ref[r].astype(F32).T.reshape(n_sp, 2, STRIP_C, CH).astype(BF16)
        for c in range(2):
            x_src[:, c, r] = turned[:, c]

    here = pl.ds(sp * rows, rows)

    def scatter_in(i, carry):
        there = (sp + i) % n_sp

        @pl.when(i > 0)
        def _():
            remote(
                x_src.at[there, core], x_dst.at[core, here], x_s.at[0], x_r.at[core], {"sp": there}
            ).start()

        remote(
            x_src.at[there, 1 - core], x_dst.at[core, here], x_s.at[1], x_r.at[core],
            {"sp": there, "tp": partner},
        ).start()
        return carry

    pl.semaphore_wait(barrier, 2 * n_sp + 1)
    lax.fori_loop(0, n_sp, scatter_in, 0)
    bias_copy = remote(bias_ref, heads.at[core], b_s.at[0], b_r.at[0], {"tp": partner})
    bias_copy.start()
    for i in range(parts):
        weights_across(0, i).start()
    x_dst[core, here] = x_src[sp, core]
    heads[core] = bias_ref[...]

    for l in range(LAYERS):
        for b in range(N_TP):
            gains[l, b] = gain_ref[l : l + 1, b * CH : (b + 1) * CH].astype(F32)
    pad[...] = jnp.zeros_like(pad)
    bias_copy.wait()
    for l in range(LAYERS):
        for h in range(HEADS):
            pad[l, h, :, :WIN_C] = heads[h // 4, l, h % 4]
    lane = lax.broadcasted_iota(jnp.int32, (8, 128), 1)
    lane_c = lane % STRIP_C
    row_c = lax.broadcasted_iota(jnp.int32, (8, 128), 0)
    nothing = jnp.full((8, 128), NEG, F32)

    def build(l, carry):
        for h in range(HEADS):
            table = pad[l, h]
            lanes = []
            for j in range(2):
                piece = table if j == 0 else pltpu.roll(table, 128 - STRIP_C, 1)
                piece = jnp.where(lane < STRIP_C, piece, 0.0)
                piece = pltpu.roll(piece, 0, 1, stride=STRIP_C, stride_axis=0)
                piece = jnp.broadcast_to(jnp.sum(piece, axis=0, keepdims=True), (8, 128))
                lanes.append(jnp.where(lane < WIN_R * STRIP_C, piece, NEG))
            straight = [pltpu.roll(g, 0, 1, stride=1, stride_axis=0) for g in lanes] + [nothing]
            carried = [nothing] + [
                pltpu.roll(g, 128 - STRIP_C, 1, stride=1, stride_axis=0) for g in lanes
            ]
            for j in range(3):
                t = jnp.where(lane_c >= row_c, straight[j], carried[j])
                for r in range(8):
                    bias[l, h, r * 8 : (r + 1) * 8, j * 128 : (j + 1) * 128] = (
                        t if r == 0 else pltpu.roll(t, r * STRIP_C, 1)
                    )
        return carry

    lax.fori_loop(0, LAYERS, build, 0)

    most = x_dst.at[core, pl.ds(0, ROWS - rows)]
    pltpu.make_async_copy(most, most, x_r.at[core]).wait()
    rest = x_dst.at[1 - core]
    pltpu.make_async_copy(rest, rest, x_r.at[1 - core]).wait()
    for g in range(GROUPS):
        for h in range(2):
            xg[0, g, y, h] = (
                x_dst[h, g * 8 : (g + 1) * 8].astype(F32).reshape(TILE, CH).astype(BF16)
            )

    to_right, to_left = right * 2 + core, left * 2 + core
    gather = (
        (y, 0, to_right), (y, 1, to_right), (left, 0, to_right),
        (y, 1, to_left), (y, 0, to_left), (right, 1, to_left),
    )

    def ag(l, g, k):
        owner, half, target = gather[k]
        ref = xg.at[l, g, owner, half]
        return remote(ref, ref, ag_s.at[g, k], ag_r.at[g, k], {"tp": target})

    sides = (opp, right, left, y)
    scatter = (
        (0, 0, to_right), (0, 1, to_left), (1, 1, to_right),
        (2, 0, to_left), (1, 0, to_right), (2, 1, to_left),
    )

    def ring(g, k):
        side, half, target = scatter[k]
        return remote(
            ssum.at[g, side, half], rs_y.at[g, k], y_s.at[g, k], y_r.at[g, k], {"tp": target}
        )

    def halo(l, g, k):
        slot = 2 * core if k else 2 * (1 - core)
        target = {"tp": partner}
        if k == 0:
            target["sp"] = (sp + 2 * core - 1 + n_sp) % n_sp
        return remote(kv.at[l, 1, g], kv.at[l, slot, g], h_s.at[l, g, k], h_r.at[l, g, k], target)

    lane_head = lax.broadcasted_iota(jnp.int32, (TILE, CH), 1) // HEAD_DIM
    ones = jnp.ones((3 * 128, 128), BF16)
    head_mask = [(lane_head == h).astype(F32).astype(BF16) for h in range(4)]

    def step_own(l, g):
        for k in (0, 3, 1, 4):
            ag(l, g, k).start()

    def step_relay(l, g):
        for k, onward in ((0, 2), (3, 5)):
            ag(l, g, k).wait_recv()
            ag(l, g, onward).start()

    def accumulate(l, g, blocks, fresh):
        total = None
        squares = None
        for chip, half in blocks:
            wide = xg[l, g, chip, half].astype(F32)
            sq_b = wide * wide
            sq_b = sq_b[:, :128] + sq_b[:, 128:]
            squares = sq_b if squares is None else squares + sq_b
            b = chip * 2 + half
            term = dot((wide * gains[l, b]).astype(BF16), wqkv[l, b])
            total = term if total is None else total + term
        if fresh:
            acc[g] = total
            sq[g] = squares
        else:
            acc[g] += total
            sq[g] += squares

    ready = set()

    def weights_in(l, which, parts_of):
        if (l, which) in ready:
            return
        ready.add((l, which))
        for i in parts_of:
            weights_here(l, i).wait()
            weights_across(l, i).wait_recv()

    def step_mine(l, g):
        weights_in(l, 0, range(3))
        accumulate(l, g, ((y, 0), (y, 1)), True)

    def step_sides(l, g):
        ag(l, g, 1).wait_recv()
        ag(l, g, 4).wait_recv()
        accumulate(l, g, ((left, 0), (right, 1), (left, 1), (right, 0)), False)

    def step_far(l, g):
        ag(l, g, 2).wait_recv()
        ag(l, g, 5).wait_recv()
        squares = sq[g]
        scaled = []
        for half in range(2):
            wide = xg[l, g, opp, half].astype(F32)
            scaled.append((wide * gains[l, opp * 2 + half]).astype(BF16))
            wide = wide * wide
            squares = squares + wide[:, :128] + wide[:, 128:]
        inverse = lax.rsqrt(jnp.sum(squares, axis=1, keepdims=True) / D + EPS)

        def total(lo, hi):
            return acc[g, :, lo:hi] + (
                dot(scaled[0], wqkv[l, opp * 2, :, lo:hi])
                + dot(scaled[1], wqkv[l, opp * 2 + 1, :, lo:hi])
            )

        kv[l, 1, g] = (total(PAIR, 3 * PAIR) * inverse).astype(BF16)
        for k in range(2):
            halo(l, g, k).start()
        qs[g] = (total(0, PAIR) * (inverse * HEAD_DIM**-0.5)).astype(BF16)
        for k in range(6):
            ag(l, g, k).wait_send()

    def window(l, slot, g, lo):
        return jnp.concatenate(
            [kv[l, slot, g, :, lo : lo + CH], kv[l, slot, (g + 1) % 4, :, lo : lo + CH]], axis=0
        )

    def step_attend(l, g):
        after = (g + 1) % 4
        for near in (g, after):
            if (l, near, "halo") not in ready:
                ready.add((l, near, "halo"))
                for k in range(2):
                    halo(l, near, k).wait_recv()
        scores, values = [], []
        for c in range(2):
            lo = c * CH
            q = jnp.concatenate(
                [qs[g, TILE // 2 :, lo : lo + CH], qs[after, : TILE // 2, lo : lo + CH]], axis=0
            )
            q_all = jnp.concatenate([q * m for m in head_mask], axis=0)
            table = bias[l, 4 * c : 4 * c + 4].reshape(4 * TILE, 3 * 128)
            scores.append(
                [dot_nt(q_all, window(l, j, g, lo)) + table[:, j * 128 : (j + 1) * 128] for j in range(3)]
            )
            values.append([window(l, j, g, PAIR + lo) for j in range(3)])
        highest = [
            jnp.max(jnp.maximum(jnp.maximum(s[0], s[1]), s[2]), axis=1, keepdims=True) for s in scores
        ]
        weights = [[jnp.exp(s - top).astype(BF16) for s in ss] for ss, top in zip(scores, highest)]
        for c in range(2):
            wide = jnp.concatenate(weights[c], axis=1)
            total = dot(wide, ones)
            o = dot(wide, jnp.concatenate(values[c], axis=0))
            o = o * (1.0 / jnp.concatenate([total, total], axis=1))
            out = o[:TILE]
            for h in range(1, 4):
                out = jnp.where(lane_head == h, o[h * TILE : (h + 1) * TILE], out)
            mixed[g, :, c * CH : (c + 1) * CH] = out.astype(BF16)
        if l < LAYERS - 1 and (l, "across") not in ready:
            ready.add((l, "across"))
            for i in range(parts):
                weights_across(l + 1, i).start()

    def chunk(l, g, k):
        piece = dot(mixed[g], wout[l, sides[k]])
        return piece[:, :CH], piece[:, CH:]

    def step_first(l, g):
        weights_in(l, 1, range(3, parts))
        for half, piece in enumerate(chunk(l, g, 0)):
            ssum[g, 0, half] = piece.astype(BF16)
        ring(g, 0).start()
        ring(g, 1).start()

    def step_rest(l, g):
        for k in (1, 2):
            for half, piece in enumerate(chunk(l, g, k)):
                ssum[g, k, half] = piece.astype(BF16)
        ring(g, 2).start()
        ring(g, 3).start()
        after = (g + 1) % 4
        for half, piece in enumerate(chunk(l, g, 3)):
            before = jnp.concatenate(
                [xg[l, g, y, half, TILE // 2 :], xg[l, after, y, half, : TILE // 2]], axis=0
            )
            own[g, half] = piece + before.astype(F32)

    def step_add(l, g):
        for k in range(2):
            ring(g, k).wait_recv()
            side = 1 + k
            ssum[g, side, k] = (ssum[g, side, k].astype(F32) + rs_y[g, k].astype(F32)).astype(BF16)
            ring(g, 4 + k).start()

    def step_finish(l, g):
        for k in (2, 3, 4, 5):
            ring(g, k).wait_recv()
        new = (
            own[g, 0] + rs_y[g, 4].astype(F32) + rs_y[g, 3].astype(F32),
            own[g, 1] + rs_y[g, 2].astype(F32) + rs_y[g, 5].astype(F32),
        )
        if l < LAYERS - 1:
            for half in range(2):
                xg[l + 1, g, y, half] = new[half].astype(BF16)
            step_own(l + 1, g)
        else:
            for half in range(2):
                o_src[half, 8 * g : 8 * g + 8] = new[half].reshape(8, STRIP_C, CH).astype(BF16)

            def send(r, carry):
                slot = 8 * g + r
                row = (slot + LAYERS * WIN_R // 2) % ROWS
                there, spot = row // rows, row % rows

                @pl.when(there != sp)
                def _():
                    remote(
                        o_src.at[core, slot], o_dst.at[core, sp, spot], o_s.at[0], o_r.at[core],
                        {"sp": there},
                    ).start()

                @pl.when(there == sp)
                def _():
                    o_dst[core, sp, spot] = o_src[core, slot]

                remote(
                    o_src.at[1 - core, slot], o_dst.at[core, sp, spot], o_s.at[1], o_r.at[core],
                    {"sp": there, "tp": partner},
                ).start()
                return carry

            lax.fori_loop(0, 8, send, 0)
        for k in range(6):
            ring(g, k).wait_send()

    steps = (
        step_own, step_relay, step_mine, step_sides, step_far,
        step_attend, step_first, step_rest, step_add, step_finish,
    )
    for step, l, g in ORDER:
        steps[step](l, g)

    for l in range(LAYERS):
        for i in range(parts):
            weights_across(l, i).wait_send()
    for l in range(LAYERS):
        for g in range(GROUPS):
            for k in range(2):
                halo(l, g, k).wait_send()
    gone = x_src.at[pl.ds(0, n_sp - 1), core]
    pltpu.make_async_copy(gone, gone, x_s.at[0]).wait()
    gone = x_src.at[:, core]
    pltpu.make_async_copy(gone, gone, x_s.at[1]).wait()
    gone = o_src.at[core, pl.ds(0, ROWS - rows)]
    pltpu.make_async_copy(gone, gone, o_s.at[0]).wait()
    gone = o_src.at[1 - core]
    pltpu.make_async_copy(gone, gone, o_s.at[1]).wait()
    most = o_dst.at[core, pl.ds(0, n_sp - 1)]
    pltpu.make_async_copy(most, most, o_r.at[core]).wait()
    rest = o_dst.at[1 - core]
    pltpu.make_async_copy(rest, rest, o_r.at[1 - core]).wait()
    for r in range(rows):
        both = jnp.stack([o_dst[c, :, r].astype(F32) for c in range(2)], axis=1)
        out_ref[r] = both.reshape(n_sp * WIN_C, CH).T.astype(BF16)


def body(token_grid, norm_gain, w_query, w_key, w_value, w_out, rel_bias):
    n_sp = lax.axis_size("sp")
    rows = token_grid.shape[0]
    wq, wk, wv = (w.reshape(LAYERS, N_TP, CH, CH) for w in (w_query, w_key, w_value))
    vmem = pl.BlockSpec(memory_space=pltpu.VMEM)
    hbm = pl.BlockSpec(memory_space=pltpu.HBM)
    dma = pltpu.SemaphoreType.DMA
    parts = 3 + CHIPS
    return pl.pallas_call(
        functools.partial(kernel, n_sp, rows),
        out_shape=jax.ShapeDtypeStruct(token_grid.shape, BF16),
        in_specs=[vmem, vmem, vmem, hbm, hbm, hbm, hbm],
        out_specs=vmem,
        scratch_shapes=[
            pltpu.VMEM((n_sp, 2, rows, STRIP_C, CH), BF16),
            pltpu.VMEM((2, ROWS, STRIP_C, CH), BF16),
            pltpu.VMEM((2, ROWS, STRIP_C, CH), BF16),
            pltpu.VMEM((2, n_sp, rows, STRIP_C, CH), BF16),
            pltpu.VMEM((LAYERS, N_TP, CH, 3 * PAIR), BF16),
            pltpu.VMEM((LAYERS, CHIPS, PAIR, PAIR), BF16),
            pltpu.VMEM((LAYERS, N_TP, 1, CH), F32),
            pltpu.VMEM((2, LAYERS, 4, WIN_R, WIN_C), F32),
            pltpu.VMEM((LAYERS, HEADS, WIN_R, 128), F32),
            pltpu.VMEM((LAYERS, HEADS, TILE, 3 * 128), F32),
            pltpu.VMEM((LAYERS, GROUPS, CHIPS, 2, TILE, CH), BF16),
            pltpu.VMEM((GROUPS, TILE, 3 * PAIR), F32),
            pltpu.VMEM((GROUPS, TILE, 128), F32),
            pltpu.VMEM((GROUPS, TILE, PAIR), BF16),
            pltpu.VMEM((LAYERS, 3, GROUPS, TILE, 2 * PAIR), BF16),
            pltpu.VMEM((GROUPS, TILE, PAIR), BF16),
            pltpu.VMEM((GROUPS, 3, 2, TILE, CH), BF16),
            pltpu.VMEM((GROUPS, 2, TILE, CH), F32),
            pltpu.VMEM((GROUPS, 6, TILE, CH), BF16),
            dma((LAYERS, parts)), dma((LAYERS, parts)), dma((LAYERS, parts)),
            dma((1,)), dma((1,)), dma((2,)), dma((2,)), dma((2,)), dma((2,)),
            dma((GROUPS, 6)), dma((GROUPS, 6)), dma((GROUPS, 6)), dma((GROUPS, 6)),
            dma((LAYERS, GROUPS, 2)), dma((LAYERS, GROUPS, 2)),
        ],
        compiler_params=pltpu.CompilerParams(
            collective_id=0, has_side_effects=True, vmem_limit_bytes=52 * 1024 * 1024
        ),
    )(token_grid, norm_gain, rel_bias, wq, wk, wv, w_out)


def solution(mesh):
    in_specs = (
        P("sp", "tp", None),
        P(),
        P(None, None, "tp"),
        P(None, None, "tp"),
        P(None, None, "tp"),
        P(None, "tp", None),
        P(None, "tp", None, None),
    )
    out_specs = P("sp", "tp", None)
    return jax.shard_map(body, mesh=mesh, in_specs=in_specs, out_specs=out_specs, check_vma=False)
```
